512 devices in a mesh: sp: 128 (over z, x, core), tp: 4 (over y).
Axes of the slice: x: 4, y: 4, z: 16, core: 2. Of those that a mesh axis runs over, the one named last changes fastest.
Arguments:
- query_main: bfloat16 [16384, 2048], P('sp', 'tp'), may hold values from -6 to 6
- query_rotary: bfloat16 [16384, 1024], P('sp', 'tp'), may hold values from -7 to 7
- latent: bfloat16 [16384, 512], P('sp'), may hold values from -24 to 24
- key_rotary: bfloat16 [16384, 64], P('sp'), may hold values from -8 to 8
- key_weight: bfloat16 [512, 2048], P(None, 'tp'), may hold values from -0.25 to 0.25
- value_weight: bfloat16 [512, 2048], P(None, 'tp'), may hold values from -0.25 to 0.25
- head_output: bfloat16 [16384, 2048], P('sp', 'tp'), may hold values from -2 to 2
- output_grad: bfloat16 [16384, 2048], P('sp', 'tp'), may hold values from -128 to 128
- row_logsum: float32 [16, 16384], P('tp', 'sp'), may hold values from 3 to 16, as said below
Outputs:
- grad_query_main: float32 [16384, 2048], P('sp', 'tp')
- grad_query_rotary: float32 [16384, 1024], P('sp', 'tp')
- grad_latent: float32 [16384, 512], P('sp')
- grad_key_rotary: float32 [16384, 64], P('sp')
- grad_key_weight: float32 [512, 2048], P('sp', 'tp')
The draws below stay inside these ranges and needn't reach their ends.
Inputs may be any that keep to these rules, and one draw needn't show every extreme that they name: With p the place of token i in its sequence and q = i % 128, row_logsum[h, i] minus the logarithm of (p + 1 + 54 (q + 1)) lies between -0.3 and 1.5.
All inputs are finite; a program needn't handle non-finite values.
Results may differ from the reference program's by a relative error of at most 0.003.
The reference program's roundings to bfloat16 on the way (of `query_latent`, `grad_rows`, `weights_low`, `dscores_low` and `mixed_low`) count: a program that leaves them out, or rounds other values in their place, can miss the bound.
Values may be sent and summed in bfloat16 or wider, within the bound.
A program may use at most 64 MiB of HBM per device.

```python
import math
import jax
import jax.numpy as jnp
from jax import lax

TOK_DEV = 128
HEADS = 16
KDIM = 128
RDIM = 64
VDIM = 128
LATENT = 512
SPAN = 32
LEAD = 8
SEQS = 5
TOKENS = 16384
N_SP = 128


own_mass = 54.0


def block_signs(key):
    picks = jax.random.randint(jax.random.fold_in(key, 7), (TOKENS // TOK_DEV, RDIM), 0, 2)
    table = picks.astype(jnp.float32) * 2.0 - 1.0
    return table[jnp.arange(TOKENS) // TOK_DEV]


def noise_field(key, shape):
    return jnp.clip(jax.random.normal(key, shape, jnp.float32), -6.0, 6.0)


def draw_query_rotary(key, part):
    signs = block_signs(key)
    noise = noise_field(jax.random.fold_in(key, 11), (TOKENS, HEADS, RDIM))
    return (noise + signs[:, None, :]).reshape(TOKENS, HEADS * RDIM).astype(jnp.bfloat16)


def draw_key_rotary(key, part):
    signs = block_signs(key)
    noise = noise_field(jax.random.fold_in(key, 13), (TOKENS, RDIM))
    strength = 4.0 * (KDIM + RDIM) ** 0.5 / RDIM
    return (noise + strength * signs).astype(jnp.bfloat16)


def draw_row_logsum(key, part):
    token = jnp.arange(TOKENS)
    device = token // TOK_DEV
    sequence = (device + LEAD) // SPAN
    first_device = jnp.maximum(sequence * SPAN - LEAD, 0)
    place = (token - first_device * TOK_DEV + 1).astype(jnp.float32)
    inside = (token % TOK_DEV + 1).astype(jnp.float32)
    total = place + own_mass * inside
    offset = jax.random.uniform(key, (HEADS, TOKENS), jnp.float32, 0.2, 1.2)
    return jnp.log(total)[None, :] + offset


def with_spikes(drawn, own_key, source, target, parts, factor):
    def block_of(axis_at):
        return (jnp.arange(drawn.shape[axis_at]) // (drawn.shape[axis_at] // parts)).reshape((-1,) + (1,) * (drawn.ndim - 1 - axis_at))

    near = jax.random.permutation(own_key, parts)[block_of(target)]
    second = (block_of(target) + parts // 2) % parts
    return jnp.where((block_of(source) == near) | (block_of(source) == second), factor * drawn, drawn)


def levels(key, shape, split, smallest, top_value):
    gain = 1.0
    for axis_at, parts in split:
        heights = jax.random.uniform(jax.random.fold_in(jax.random.fold_in(key, 6), axis_at), (parts,), jnp.float32, smallest / len(split), top_value / len(split))
        gain = gain * jnp.repeat(jnp.exp(heights), shape[axis_at] // parts).reshape((-1,) + (1,) * (len(shape) - 1 - axis_at))
    return gain


def centred(stream_key, extent, scale, bound, pieces=(), held_as=jnp.bfloat16):
    entries = jax.random.normal(stream_key, extent, jnp.float32) * scale
    if len(pieces) > 0:
        entries = levels(stream_key, extent, pieces, -0.22, 0.18) * entries
    return jnp.clip(entries, min=-bound, max=bound).astype(held_as)


def noise_with(own_key, shape, spread, most, split, heavy, held_as=jnp.bfloat16):
    entries = spread * jax.random.normal(own_key, shape, jnp.float32)
    if split:
        entries = entries * levels(own_key, shape, split, -0.22, 0.18)
    return jnp.clip(with_spikes(entries, jax.random.fold_in(own_key, 3), *heavy), -most, most).astype(held_as)


def setup_inputs(seed: int = 0) -> dict:
    seeds = jax.random.split(jax.random.key(seed), 10)
    query_main = centred(seeds[0], (TOKENS, HEADS * KDIM), 1.0, 6.0, ((0, 128), (1, 4)))
    query_rotary = draw_query_rotary(jax.random.fold_in(seeds[9], 71), 0)
    latent = noise_with(seeds[2], (TOKENS, LATENT), 1.0, 24.0, ((0, 128),), (0, 1, 128, 5.5))
    key_rotary = draw_key_rotary(jax.random.fold_in(seeds[9], 71), 0)
    key_weight = centred(seeds[4], (LATENT, HEADS * KDIM), LATENT ** -0.5, 0.25, ((1, 4),))
    value_weight = centred(seeds[5], (LATENT, HEADS * VDIM), LATENT ** -0.5, 0.25, ((1, 4),))
    head_output = centred(seeds[6], (TOKENS, HEADS * VDIM), 0.3, 2.0, ((0, 128), (1, 4)))
    output_grad = noise_with(seeds[7], (TOKENS, HEADS * VDIM), 6.0, 128.0, ((0, 128), (1, 4)), (0, 1, 128, 5.5))
    row_logsum = draw_row_logsum(jax.random.fold_in(seeds[9], 71), 0)
    return {"query_main": query_main, "query_rotary": query_rotary, "latent": latent, "key_rotary": key_rotary, "key_weight": key_weight, "value_weight": value_weight, "head_output": head_output, "output_grad": output_grad, "row_logsum": row_logsum}


def sequence_grads(lat_seq, rot_seq, query_latent, grad_rows, rot_query, row_logs, row_terms, factor, width):
    wide = jnp.float32
    blocks = lat_seq.shape[0] // width
    heads = query_latent.shape[1]
    lat_all = lat_seq.astype(wide)
    rot_all = rot_seq.astype(wide)
    qlat_all = query_latent.astype(wide)
    grows_all = grad_rows.astype(wide)
    qrot_all = rot_query.astype(wide)

    def query_block(carry, query_index):
        acc_lat, acc_rot = carry
        query_start = (query_index * width).astype(jnp.int32)
        qlat = lax.dynamic_slice_in_dim(qlat_all, query_start, width, 0)
        grows = lax.dynamic_slice_in_dim(grows_all, query_start, width, 0)
        qrot = lax.dynamic_slice_in_dim(qrot_all, query_start, width, 0)
        logs = lax.dynamic_slice_in_dim(row_logs, query_start, width, 0)
        terms = lax.dynamic_slice_in_dim(row_terms, query_start, width, 0)
        query_place = query_start + jnp.arange(width, dtype=jnp.int32)

        def key_block(key_index, inner):
            def visit(state):
                mixed_sum, rot_sum, acc_lat, acc_rot = state
                key_start = (key_index * width).astype(jnp.int32)
                lat_block = lax.dynamic_slice_in_dim(lat_all, key_start, width, 0)
                rot_block = lax.dynamic_slice_in_dim(rot_all, key_start, width, 0)
                key_place = key_start + jnp.arange(width, dtype=jnp.int32)
                seen = key_place[None, :] <= query_place[:, None]
                scores = jnp.einsum("thl,kl->thk", qlat, lat_block) + jnp.einsum("thr,kr->thk", qrot, rot_block)
                weights = jnp.where(seen[:, None, :], jnp.exp(factor * scores - logs[:, :, None]), 0.0)
                slopes = jnp.einsum("thl,kl->thk", grows, lat_block)
                dscores = weights * (slopes - terms[:, :, None])
                weights_low = lax.optimization_barrier(weights.astype(jnp.bfloat16)).astype(wide)
                dscores_low = lax.optimization_barrier(dscores.astype(jnp.bfloat16)).astype(wide)
                mixed_sum = mixed_sum + jnp.einsum("thk,kl->thl", dscores_low, lat_block)
                rot_sum = rot_sum + jnp.einsum("thk,kr->thr", dscores_low, rot_block)
                part_lat = factor * jnp.einsum("thk,thl->kl", dscores_low, qlat) + jnp.einsum("thk,thl->kl", weights_low, grows)
                part_rot = factor * jnp.einsum("thk,thr->kr", dscores_low, qrot)
                old_lat = lax.dynamic_slice_in_dim(acc_lat, key_start, width, 0)
                old_rot = lax.dynamic_slice_in_dim(acc_rot, key_start, width, 0)
                acc_lat = lax.dynamic_update_slice_in_dim(acc_lat, old_lat + part_lat, key_start, 0)
                acc_rot = lax.dynamic_update_slice_in_dim(acc_rot, old_rot + part_rot, key_start, 0)
                return mixed_sum, rot_sum, acc_lat, acc_rot

            def keep(state):
                return state

            return lax.cond(key_index <= query_index, visit, keep, inner)

        start_state = (jnp.zeros((width, heads, lat_all.shape[1]), wide), jnp.zeros((width, heads, rot_all.shape[1]), wide), acc_lat, acc_rot)
        mixed_sum, rot_sum, acc_lat, acc_rot = lax.fori_loop(0, blocks, key_block, start_state)
        return (acc_lat, acc_rot), (mixed_sum, rot_sum)

    start = (jnp.zeros(lat_seq.shape, wide), jnp.zeros(rot_seq.shape, wide))
    (acc_lat, acc_rot), (mixed_parts, rot_parts) = lax.scan(query_block, start, jnp.arange(blocks, dtype=jnp.int32))
    mixed = mixed_parts.reshape(lat_seq.shape[0], heads, lat_seq.shape[1])
    rot_sum = rot_parts.reshape(lat_seq.shape[0], heads, rot_seq.shape[1])
    return mixed, rot_sum, acc_lat, acc_rot


def reference(query_main, query_rotary, latent, key_rotary, key_weight, value_weight, head_output, output_grad, row_logsum):
    wide = jnp.float32
    factor = (KDIM + RDIM) ** -0.5
    count = latent.shape[0]
    width = math.gcd(LEAD * TOK_DEV, 512)
    main_query = query_main.reshape(count, HEADS, KDIM).astype(wide)
    rot_query = query_rotary.reshape(count, HEADS, RDIM)
    key_proj = key_weight.reshape(LATENT, HEADS, KDIM).astype(wide)
    value_proj = value_weight.reshape(LATENT, HEADS, VDIM).astype(wide)
    grad_heads = output_grad.reshape(count, HEADS, VDIM).astype(wide)
    query_latent = jnp.einsum("thd,lhd->thl", main_query, key_proj).astype(jnp.bfloat16)
    grad_rows = jnp.einsum("thd,lhd->thl", grad_heads, value_proj).astype(jnp.bfloat16)
    row_terms = jnp.sum(head_output.reshape(count, HEADS, VDIM).astype(wide) * grad_heads, axis=2)
    row_logs = row_logsum.T.astype(wide)
    mixed_list, rot_list, lat_list, key_rot_list = [], [], [], []
    for sequence in range(SEQS):
        first = max(sequence * SPAN - LEAD, 0) * TOK_DEV
        last = min((sequence + 1) * SPAN - LEAD, N_SP) * TOK_DEV
        mixed, rot_sum, acc_lat, acc_rot = sequence_grads(
            latent[first:last], key_rotary[first:last], query_latent[first:last], grad_rows[first:last],
            rot_query[first:last], row_logs[first:last], row_terms[first:last], factor, width)
        mixed_list.append(mixed)
        rot_list.append(rot_sum)
        lat_list.append(acc_lat)
        key_rot_list.append(acc_rot)
    mixed = jnp.concatenate(mixed_list, axis=0)
    rot_sum = jnp.concatenate(rot_list, axis=0)
    grad_latent = jnp.concatenate(lat_list, axis=0)
    grad_key_rotary = jnp.concatenate(key_rot_list, axis=0)
    mixed_low = lax.optimization_barrier(mixed.astype(jnp.bfloat16)).astype(wide)
    grad_query_main = (factor * jnp.einsum("thl,lhd->thd", mixed_low, key_proj)).reshape(count, HEADS * KDIM)
    grad_query_rotary = (factor * rot_sum).reshape(count, HEADS * RDIM)
    grad_key_weight = (factor * jnp.einsum("thl,thd->lhd", mixed_low, main_query)).reshape(LATENT, HEADS * KDIM)
    return (grad_query_main, grad_query_rotary, grad_latent, grad_key_rotary, grad_key_weight)
```

```python
import functools

import jax
import jax.numpy as jnp
from jax import lax
from jax.experimental import pallas as pl
from jax.experimental.pallas import tpu as pltpu
from jax.sharding import Mesh
from jax.sharding import PartitionSpec as P

MESH = pl.DeviceIdType.MESH
SP = ("z", "x", "c")
F32 = jnp.float32
BF16 = jnp.bfloat16
WIDE = 640
NT = (((1,), (1,)), ((), ()))
TN = (((0,), (0,)), ((), ()))


def dot(a, b, dims=(((1,), (0,)), ((), ()))):
    return lax.dot_general(a, b, dims, preferred_element_type=F32)


def body(
    qm, qr, kcat, kw, vw, ho, og, ls,
    o_main, o_rot, o_lat, o_krot, o_weight,
    keys, part, dsum, y1s, y1r, y2s, y2r, xs, xr, zs, zr, fin,
    mix, qc, gr, stats, low, term, termr, wx0, wxs, wxr, wz, wzr, wf, wfr,
    s_loc, s_kz, r_kz, s_kx, r_kx, s_kd, r_kd, s_d, r_d, s_y1, r_y1, s_y2, r_y2,
    s_x, r_x, s_z, r_z, s_f, r_f, s_t, r_t, s_wx, r_wx, s_wz, r_wz, s_wf, r_wf,
):
    z, x, c, y = (lax.axis_index(a) for a in ("z", "x", "c", "y"))
    factor = 192.0 ** (-0.5)
    zp = jnp.where(z < 3, z, (z + 1) % 4)
    planes = jnp.where(z < 3, 3, jnp.where(z < 15, 4, 1))
    more = planes - 1 - zp
    sib = {"c": 1 - c}
    x1, x3, x2 = x + 1 - 2 * (x % 2), 3 - x, (x + 2) % 4
    y1, y3, y2 = y + 1 - 2 * (y % 2), 3 - y, (y + 2) % 4

    def remote(src, dst, ss, rs, dev):
        return pltpu.make_async_remote_copy(
            src_ref=src, dst_ref=dst, send_sem=ss, recv_sem=rs, device_id=dev, device_id_type=MESH
        )

    def c_kz(s):
        return remote(keys.at[s, 0, 0], keys.at[s + 1, 0, 0], s_kz.at[s], r_kz.at[s + 1], {"z": z + 1})

    def c_kzr(s):
        return remote(keys.at[s, 0, 0], keys.at[s, 0, 0], s_kz.at[s], r_kz.at[s], {"z": z - 1})

    def c_kx(s, j):
        dev = {"x": x1} if j == 1 else {"x": x3}
        return remote(keys.at[s, 0, 0], keys.at[s, j, 0], s_kx.at[s, j - 1], r_kx.at[s, j - 1], dev)

    def c_kh(s, j):
        src, rows, dev = (1, 0, {"x": x3}) if j == 0 else (2, 64, {"x": x1})
        return remote(
            keys.at[s, src, 0, pl.ds(rows, 64)], keys.at[s, 3, 0, pl.ds(rows, 64)],
            s_kx.at[s, 2 + j], r_kx.at[s, 2 + j], dev,
        )

    def c_kd(s, j):
        return remote(keys.at[s, j, 0], keys.at[s, j, 1], s_kd.at[s, j], r_kd.at[s, j], sib)

    def c_d(s, j):
        return remote(part.at[s, j, 1], dsum.at[s, j], s_d.at[s, j], r_d.at[s, j], sib)

    def c_y1(s, g):
        dev = {"y": y1} if g == 0 else {"y": y3}
        return remote(y1s.at[s, g], y1r.at[s, g], s_y1.at[s, g], r_y1.at[s, g], dev)

    def c_y2(s, g):
        dev = {"y": y3} if g == 0 else {"y": y1}
        return remote(y2s.at[s, g], y2r.at[s, g], s_y2.at[s, g], r_y2.at[s, g], dev)

    def c_x(s, j):
        dev = {"x": (x1, x3, x2)[j - 1]}
        return remote(xs.at[s, j], xr.at[s, j], s_x.at[s, j], r_x.at[s, j], dev)

    def c_z(s):
        return remote(zs.at[s], zr.at[s], s_z.at[s], r_z.at[s], {"z": z - s})

    def c_zr(s):
        return remote(zs.at[s], zr.at[s], s_z.at[s], r_z.at[s], {"z": z + s})

    def c_f(j):
        dev = {"y": (y1, y3, y2)[j - 1]}
        return remote(fin.at[0], fin.at[j], s_f.at[j], r_f.at[j], dev)

    c_t = remote(term.at[1], termr, s_t, r_t, sib)

    def c_wx(j):
        dev = {"x": (x1, x3, x2)[j - 1]}
        return remote(wxs.at[j], wxr.at[j], s_wx.at[j], r_wx.at[j], dev)

    def c_wz(d):
        to = (z + d) % 16
        return remote(wz.at[to], wzr.at[d], s_wz.at[d], r_wz.at[d], {"z": to})

    c_wf = remote(wf, wfr, s_wf, r_wf, sib)

    load = pltpu.make_async_copy(kcat, keys.at[0, 0, 0], s_loc)
    load.start()
    barrier = pltpu.get_barrier_semaphore()
    for dev in (sib, {"x": x1}, {"x": x2}, {"x": x3}, {"y": y1}, {"y": y2}, {"y": y3}):
        pl.semaphore_signal(barrier, inc=1, device_id=dev, device_id_type=MESH)

    def greet(d, carry):
        pl.semaphore_signal(barrier, inc=1, device_id={"z": (z + d) % 16}, device_id_type=MESH)
        return carry

    lax.fori_loop(1, 16, greet, 0)
    load.wait()
    pl.semaphore_wait(barrier, 22)

    def pass_on(s):
        @pl.when(more > 0)
        def _():
            c_kz(s).start()

        c_kx(s, 1).start()
        c_kx(s, 2).start()
        c_kd(s, 0).start()

    pass_on(0)

    ones = jnp.ones((8, 128), F32)
    for h in range(4):
        cols = pl.ds(h * 128, 128)
        rows = pl.ds(h * 128, 128)
        qc[rows, 0:512] = dot(qm[:, cols], kw[:, cols], NT).astype(BF16)
        gr[rows, :] = dot(og[:, cols], vw[:, cols], NT).astype(BF16)
        rot = qr[:, h * 64 : (h + 1) * 64]
        qc[rows, 512:WIDE] = jnp.concatenate([rot, jnp.zeros((128, 64), BF16)], axis=1)
        prod = ho[:, cols].astype(F32) * og[:, cols].astype(F32)
        sums = lax.dot_general(
            ones, prod, NT, precision=lax.Precision.HIGHEST, preferred_element_type=F32
        )
        stats[1:2, cols] = sums[0:1, :]
        stats[0:1, cols] = ls[h : h + 1, :]
    mix[...] = jnp.zeros_like(mix)

    def tile(s, j):
        kt = keys[s, j].reshape(256, WIDE)
        turn = jnp.where(j == 0, x, jnp.where(j == 1, x1, jnp.where(j == 2, x3, x2)))
        far = jnp.where(s > 0, 1 << 20, 0)
        first = (2 * turn + c) * 128 - far
        second = (2 * turn + 1 - c) * 128 - 128 - far
        k_row = lax.broadcasted_iota(jnp.int32, (256, 1), 0)
        k_place = jnp.where(k_row < 128, k_row + first, k_row + second)
        q_place = lax.broadcasted_iota(jnp.int32, (1, 512), 1) % 128 + (2 * x + c) * 128
        scores = dot(kt, qc[...], NT)
        weights = jnp.where(k_place <= q_place, jnp.exp(factor * scores - stats[0:1, :]), 0.0)
        slopes = dot(kt[:, 0:512], gr[...], NT)
        dscores = weights * (slopes - stats[1:2, :])
        w_low = weights.astype(BF16)
        d_low = dscores.astype(BF16)
        mix[...] += dot(kt, d_low, TN)
        main = factor * dot(d_low, qc[:, 0:512]) + dot(w_low, gr[...])
        rest = factor * dot(d_low, qc[:, 512:WIDE])
        part[s, j, :, :, 0:512] = main.reshape(2, 128, 512)
        part[s, j, :, :, 512:WIDE] = rest.reshape(2, 128, 128)

    def own(s, j, yy):
        rows = pl.ds(pl.multiple_of(yy * 32, 32), 32)
        return part[s, j, 0, rows, :] + dsum[s, j, rows, :]

    def do_y1(s, g):
        pair = (2 * g, 2 * g + 1)
        for j in pair:
            c_d(s, j).wait_recv()
        for i, j in enumerate(pair):
            y1s[s, g, 0, i] = own(s, j, y1 if g == 0 else y3).astype(BF16)
            y1s[s, g, 1, i] = own(s, j, y2).astype(BF16)
        c_y1(s, g).start()

    def do_y2(s, g):
        c_y1(s, g).wait_recv()
        for i, j in enumerate((2 * g, 2 * g + 1)):
            y2s[s, g, i] = own(s, j, y3 if g == 0 else y1) + y1r[s, g, 1, i].astype(F32)
        c_y2(s, g).start()

    def do_x(s, g):
        c_y2(s, g).wait_recv()
        for i, j in enumerate((2 * g, 2 * g + 1)):
            xs[s, j] = own(s, j, y) + y1r[s, g, 0, i].astype(F32) + y2r[s, g, i]
            if j > 0:
                c_x(s, j).start()

    def do_z(s):
        for j in (1, 2, 3):
            c_x(s, j).wait_recv()
        zs[s] = xs[s, 0] + xr[s, 1] + xr[s, 2] + xr[s, 3]

        @pl.when(s > 0)
        def _():
            c_z(s).start()

    def visit(t, carry):
        def at(offset, act):
            s = (t - offset + 16) // 4 - 4

            @pl.when(((t - offset + 16) % 4 == 0) & (s >= 0) & (s <= zp))
            def _():
                act(s)

        def act_a(s):
            @pl.when(s > 0)
            def _():
                c_kzr(s).wait_recv()
                pass_on(s)

        def act_b(s):
            c_kx(s, 1).wait_recv()
            c_kx(s, 2).wait_recv()
            c_kh(s, 0).start()
            c_kh(s, 1).start()
            c_kd(s, 1).start()
            c_kd(s, 2).start()

        def act_c(s):
            c_kh(s, 0).wait_recv()
            c_kh(s, 1).wait_recv()
            c_kd(s, 3).start()

        at(0, act_b)
        at(-4, act_a)
        at(2, act_c)
        at(13, do_z)
        at(11, lambda s: do_x(s, 1))
        at(9, lambda s: do_x(s, 0))
        at(8, lambda s: do_y2(s, 1))
        at(6, lambda s: do_y2(s, 0))
        at(5, lambda s: do_y1(s, 1))
        at(3, lambda s: do_y1(s, 0))

        @pl.when(t < 4 * zp + 4)
        def _():
            s, j = t // 4, t % 4
            c_kd(s, j).wait_recv()
            tile(s, j)
            c_d(s, j).start()

        over = t - (4 * zp + 4)

        @pl.when(over == 0)
        def _():
            low[...] = mix[0:512, :].astype(BF16)
            for rel in (1, 0):
                half = c if rel == 0 else 1 - c
                for hh in (0, 1):
                    cols = pl.ds(pl.multiple_of((2 * half + hh) * 128, 128), 128)
                    got = factor * dot(low[:, cols], qm[:, cols])
                    term[rel, :, :, :, hh * 128 : (hh + 1) * 128] = got.reshape(16, 4, 8, 128)
                if rel == 1:
                    c_t.start()

        @pl.when(over == 1)
        def _():
            c_t.wait_recv()
            for j in range(4):
                turn = (x, x1, x3, x2)[j]
                got = (term[0, :, turn] + termr[:, turn]).reshape(128, 256)
                if j == 0:
                    wx0[...] = got
                else:
                    wxs[j] = got.astype(BF16)
                    c_wx(j).start()
            for h in range(4):
                cols = pl.ds(h * 128, 128)
                o_main[:, cols] = factor * dot(low[:, cols], kw[:, cols], TN)
            for g in range(2):
                a = mix[512:640, pl.ds(g * 256, 128)].T
                b = mix[512:640, pl.ds(g * 256 + 128, 128)].T
                o_rot[:, pl.ds(g * 128, 128)] = factor * jnp.concatenate([a[:, 0:64], b[:, 0:64]], axis=1)

        @pl.when(over == 3)
        def _():
            got = wx0[...]
            for j in (1, 2, 3):
                c_wx(j).wait_recv()
                got = got + wxr[j].astype(F32)
            wz[...] = got.reshape(16, 8, 256)

            def go(d, carry):
                c_wz(d).start()
                return carry

            lax.fori_loop(1, 16, go, 0)

        return carry

    lax.fori_loop(0, 4 * zp + 14, visit, 0)

    def wait_z(d, carry):
        c_zr(d).wait_recv()
        zs[0] += zr[d]
        return carry

    lax.fori_loop(1, more + 1, wait_z, 0)
    fin[0] = zs[0]
    for j in (1, 2, 3):
        c_f(j).start()

    def wait_wz(d, total):
        c_wz(d).wait_recv()
        return total + wzr[d]

    wf[...] = lax.fori_loop(1, 16, wait_wz, wz[z])
    c_wf.start()

    for j in range(4):
        if j > 0:
            c_f(j).wait_recv()
        rows = pl.ds(pl.multiple_of((y, y1, y3, y2)[j] * 32, 32), 32)
        o_lat[rows, :] = fin[j, :, 0:512]
        o_krot[rows, :] = fin[j, :, 512:576]
    c_wf.wait_recv()

    @pl.when(c == 0)
    def _():
        o_weight[:, 0:256] = wf[0:4, :]
        o_weight[:, 256:512] = wfr[0:4, :]

    @pl.when(c == 1)
    def _():
        o_weight[:, 0:256] = wfr[4:8, :]
        o_weight[:, 256:512] = wf[4:8, :]

    def drain(s, carry):
        @pl.when(more > 0)
        def _():
            c_kz(s).wait_send()

        for j in (1, 2):
            c_kx(s, j).wait_send()
        for j in (0, 1):
            c_kh(s, j).wait_send()
            c_y1(s, j).wait_send()
            c_y2(s, j).wait_send()
        for j in range(4):
            c_kd(s, j).wait_send()
            c_d(s, j).wait_send()
            if j > 0:
                c_x(s, j).wait_send()

        @pl.when(s > 0)
        def _():
            c_z(s).wait_send()

        return carry

    lax.fori_loop(0, zp + 1, drain, 0)
    c_t.wait_send()
    c_wf.wait_send()
    for j in (1, 2, 3):
        c_wx(j).wait_send()
        c_f(j).wait_send()

    def drain_wz(d, carry):
        c_wz(d).wait_send()
        return carry

    lax.fori_loop(1, 16, drain_wz, 0)


def per_device(query_main, query_rotary, latent, key_rotary, key_weight, value_weight, head_output, output_grad, row_logsum):
    kcat = jnp.concatenate([latent, key_rotary, jnp.zeros((128, 64), BF16)], axis=1)
    v = pl.BlockSpec(memory_space=pltpu.VMEM)
    hbm = pl.BlockSpec(memory_space=pl.ANY)
    dma = pltpu.SemaphoreType.DMA
    scratch = [
        pltpu.VMEM((5, 4, 2, 128, WIDE), BF16),
        pltpu.VMEM((4, 4, 2, 128, WIDE), F32),
        pltpu.VMEM((4, 4, 128, WIDE), F32),
        pltpu.VMEM((4, 2, 2, 2, 32, WIDE), BF16),
        pltpu.VMEM((4, 2, 2, 2, 32, WIDE), BF16),
        pltpu.VMEM((4, 2, 2, 32, WIDE), F32),
        pltpu.VMEM((4, 2, 2, 32, WIDE), F32),
        pltpu.VMEM((4, 4, 32, WIDE), F32),
        pltpu.VMEM((4, 4, 32, WIDE), F32),
        pltpu.VMEM((4, 32, WIDE), F32),
        pltpu.VMEM((4, 32, WIDE), F32),
        pltpu.VMEM((4, 32, WIDE), F32),
        pltpu.VMEM((WIDE, 512), F32),
        pltpu.VMEM((512, WIDE), BF16),
        pltpu.VMEM((512, 512), BF16),
        pltpu.VMEM((8, 512), F32),
        pltpu.VMEM((512, 512), BF16),
        pltpu.VMEM((2, 16, 4, 8, 256), F32),
        pltpu.VMEM((16, 4, 8, 256), F32),
        pltpu.VMEM((128, 256), F32),
        pltpu.VMEM((4, 128, 256), BF16),
        pltpu.VMEM((4, 128, 256), BF16),
        pltpu.VMEM((16, 8, 256), F32),
        pltpu.VMEM((16, 8, 256), F32),
        pltpu.VMEM((8, 256), F32),
        pltpu.VMEM((8, 256), F32),
        dma,
        dma((5,)), dma((5,)),
        dma((4, 4)), dma((4, 4)),
        dma((4, 4)), dma((4, 4)),
        dma((4, 4)), dma((4, 4)),
        dma((4, 2)), dma((4, 2)),
        dma((4, 2)), dma((4, 2)),
        dma((4, 4)), dma((4, 4)),
        dma((4,)), dma((4,)),
        dma((4,)), dma((4,)),
        dma, dma,
        dma((4,)), dma((4,)),
        dma((16,)), dma((16,)),
        dma, dma,
    ]
    return pl.pallas_call(
        body,
        out_shape=(
            jax.ShapeDtypeStruct((128, 512), F32),
            jax.ShapeDtypeStruct((128, 256), F32),
            jax.ShapeDtypeStruct((128, 512), F32),
            jax.ShapeDtypeStruct((128, 64), F32),
            jax.ShapeDtypeStruct((4, 512), F32),
        ),
        in_specs=[v, v, hbm, v, v, v, v, v],
        out_specs=(v,) * 5,
        scratch_shapes=scratch,
        compiler_params=pltpu.CompilerParams(
            collective_id=0, has_side_effects=True, vmem_limit_bytes=60 * 1024 * 1024
        ),
    )(query_main, query_rotary, kcat, key_weight, value_weight, head_output, output_grad, row_logsum)


def solution(mesh):
    finer = Mesh(mesh.devices.reshape(16, 4, 2, mesh.shape["tp"]), ("z", "x", "c", "y"))
    return jax.shard_map(
        per_device,
        mesh=finer,
        in_specs=(
            P(SP, "y"),
            P(SP, "y"),
            P(SP, None),
            P(SP, None),
            P(None, "y"),
            P(None, "y"),
            P(SP, "y"),
            P(SP, "y"),
            P("y", SP),
        ),
        out_specs=(P(SP, "y"), P(SP, "y"), P(SP, None), P(SP, None), P(SP, "y")),
        check_vma=False,
    )
```

```python
import jax
import jax.numpy as jnp
from jax import lax
from jax.experimental import pallas as pl
from jax.experimental.pallas import tpu as pltpu
from jax.sharding import Mesh
from jax.sharding import PartitionSpec as P

MESH = pl.DeviceIdType.MESH
SP = ("z", "x", "c")
F32 = jnp.float32
BF16 = jnp.bfloat16
WIDE = 640
NT = (((1,), (1,)), ((), ()))
TN = (((0,), (0,)), ((), ()))


def dot(a, b, dims=(((1,), (0,)), ((), ()))):
    return lax.dot_general(a, b, dims, preferred_element_type=F32)


ORDER_S = (0, 1, 0, 0, 1, 1, 2, 2, 2, 0, 1, 2, 3, 3, 3, 3)
ORDER_J = (0, 0, 1, 2, 1, 2, 0, 1, 2, 3, 3, 3, 3, 1, 2, 0)


def pick(table, t):
    out = jnp.int32(0)
    for k, v in enumerate(table):
        if v:
            out = out + jnp.where(t == k, v, 0)
    return out


def body(
    qm, qr, lat, krt, kw, vw, ho, og, ls,
    o_main, o_rot, o_lat, o_krot, o_weight,
    qb, st, qc, gr, keys, mix, part, dsum, y1s, y1r, y2s, y2r, zs, zr, fin,
    dqs, dqh, dqr, term, termr, wx0, wxs, wxr, wz, wzr, wf, wfr,
    s_loc, s_q, r_q, s_st, r_st, s_kz, r_kz, s_kd, r_kd, s_d, r_d, s_y1, r_y1, s_y2, r_y2,
    s_z, r_z, s_f, r_f, s_dh, r_dh, s_dq, r_dq, s_t, r_t, s_wx, r_wx, s_wz, r_wz, s_wf, r_wf,
):
    z, x, c, y = (lax.axis_index(a) for a in ("z", "x", "c", "y"))
    factor = 192.0 ** (-0.5)
    zp = jnp.where(z < 3, z, (z + 1) % 4)
    planes = jnp.where(z < 3, 3, jnp.where(z < 15, 4, 1))
    more = planes - 1 - zp
    sib = {"c": 1 - c}
    x1, x3, x2 = x + 1 - 2 * (x % 2), 3 - x, (x + 2) % 4
    y1, y3, y2 = y + 1 - 2 * (y % 2), 3 - y, (y + 2) % 4
    xdev = (None, {"x": x1}, {"x": x3}, {"x": x2})
    ydev = (None, {"y": y1}, {"y": y3}, {"y": y2})

    def remote(src, dst, ss, rs, dev):
        return pltpu.make_async_remote_copy(
            src_ref=src, dst_ref=dst, send_sem=ss, recv_sem=rs, device_id=dev, device_id_type=MESH
        )

    def c_q(j):
        return remote(qb.at[0], qb.at[j], s_q.at[j], r_q.at[j], xdev[j])

    def c_qh(i):
        rows = pl.ds(64 * i, 64)
        return remote(qb.at[1 + i, rows], qb.at[3, rows], s_q.at[3 + i], r_q.at[3 + i], xdev[2 - i])

    def c_st(j):
        return remote(st.at[0], st.at[j], s_st.at[j], r_st.at[j], xdev[j])

    def c_kz(s):
        return remote(keys.at[s, 0], keys.at[s + 1, 0], s_kz.at[s], r_kz.at[s + 1], {"z": z + 1})

    def c_kzr(s):
        return remote(keys.at[s, 0], keys.at[s, 0], s_kz.at[s], r_kz.at[s], {"z": z - 1})

    def c_kd(s):
        return remote(keys.at[s, 0], keys.at[s, 1], s_kd.at[s], r_kd.at[s], sib)

    def c_d(s):
        return remote(part.at[s, 1], dsum.at[s], s_d.at[s], r_d.at[s], sib)

    def c_y1(s, g):
        return remote(y1s.at[s, g], y1r.at[s, g], s_y1.at[s, g], r_y1.at[s, g], ydev[1 + g])

    def c_y2(s, g):
        return remote(y2s.at[s, g], y2r.at[s, g], s_y2.at[s, g], r_y2.at[s, g], ydev[2 - g])

    def c_z(s):
        return remote(zs.at[s], zr.at[s], s_z.at[s], r_z.at[s], {"z": z - s})

    def c_zr(s):
        return remote(zs.at[s], zr.at[s], s_z.at[s], r_z.at[s], {"z": z + s})

    def c_f(j):
        return remote(fin.at[0], fin.at[j], s_f.at[j], r_f.at[j], ydev[j])

    def c_dh(i):
        rows = pl.ds(64 * i, 64)
        return remote(dqs.at[3, rows], dqh.at[i], s_dh.at[i], r_dh.at[i], xdev[1 + i])

    def c_dq(j):
        return remote(dqs.at[j], dqr.at[j - 1], s_dq.at[j], r_dq.at[j], xdev[j])

    c_t = remote(term.at[1], termr, s_t, r_t, sib)

    def c_wx(j):
        return remote(wxs.at[j], wxr.at[j], s_wx.at[j], r_wx.at[j], xdev[j])

    def c_wz(d):
        to = (z + d) % 16
        return remote(wz.at[to], wzr.at[d], s_wz.at[d], r_wz.at[d], {"z": to})

    c_wf = remote(wf, wfr, s_wf, r_wf, sib)

    loads = [
        pltpu.make_async_copy(qm, qb.at[0, :, 0:512], s_loc.at[0]),
        pltpu.make_async_copy(qr, qb.at[0, :, 512:768], s_loc.at[1]),
        pltpu.make_async_copy(og, qb.at[0, :, 768:1280], s_loc.at[2]),
        pltpu.make_async_copy(lat, keys.at[0, 0, :, 0:512], s_loc.at[3]),
    ]
    for copy in loads:
        copy.start()
    barrier = pltpu.get_barrier_semaphore()
    for dev in (sib, *xdev[1:], *ydev[1:]):
        pl.semaphore_signal(barrier, inc=1, device_id=dev, device_id_type=MESH)

    def greet(d, carry):
        pl.semaphore_signal(barrier, inc=1, device_id={"z": (z + d) % 16}, device_id_type=MESH)
        return carry

    lax.fori_loop(1, 16, greet, 0)
    keys[0, 0, :, 512:WIDE] = jnp.concatenate([krt[...].T, jnp.zeros((128, 64), BF16)], axis=1)
    for copy in loads:
        copy.wait()
    pl.semaphore_wait(barrier, 22)

    def pass_on(s):
        @pl.when(more > 0)
        def _():
            c_kz(s).start()

        c_kd(s).start()

    c_q(1).start()
    c_q(2).start()
    pass_on(0)

    ones = jnp.ones((8, 128), F32)
    for h in range(4):
        cols = pl.ds(h * 128, 128)
        prod = ho[:, cols].astype(F32) * qb[0, :, 768 + h * 128 : 896 + h * 128].astype(F32)
        sums = lax.dot_general(
            ones, prod, NT, precision=lax.Precision.HIGHEST, preferred_element_type=F32
        )
        st[0, 1:2, cols] = sums[0:1, :]
        st[0, 0:1, cols] = ls[h : h + 1, :]
    for j in (1, 2, 3):
        c_st(j).start()

    def project(j):
        for h in range(4):
            cols = pl.ds(h * 128, 128)
            rows = pl.ds(h * 128, 128)
            qc[j, rows, 0:512] = dot(qb[j, :, h * 128 : h * 128 + 128], kw[:, cols], NT).astype(BF16)
            gr[j, rows, :] = dot(qb[j, :, 768 + h * 128 : 896 + h * 128], vw[:, cols], NT).astype(BF16)
            rot = qb[j, :, 512 + h * 64 : 576 + h * 64]
            qc[j, rows, 512:WIDE] = jnp.concatenate([rot, jnp.zeros((128, 64), BF16)], axis=1)

    project(0)
    mix[...] = jnp.zeros_like(mix)
    part[...] = jnp.zeros_like(part)

    def tile(s, j):
        kt = keys[s].reshape(256, WIDE)
        turn = jnp.where(j == 0, x, jnp.where(j == 1, x1, jnp.where(j == 2, x3, x2)))
        far = jnp.where(s > 0, 1 << 20, 0)
        first = (2 * x + c) * 128 - far
        second = (2 * x + 1 - c) * 128 - 128 - far
        k_row = lax.broadcasted_iota(jnp.int32, (256, 1), 0)
        k_place = jnp.where(k_row < 128, k_row + first, k_row + second)
        q_place = lax.broadcasted_iota(jnp.int32, (1, 512), 1) % 128 + (2 * turn + c) * 128
        scores = dot(kt, qc[j], NT)
        weights = jnp.where(k_place <= q_place, jnp.exp(factor * scores - st[j, 0:1, :]), 0.0)
        slopes = dot(kt[:, 0:512], gr[j], NT)
        dscores = weights * (slopes - st[j, 1:2, :])
        w_low = weights.astype(BF16)
        d_low = dscores.astype(BF16)
        mix[j] += dot(kt, d_low, TN)
        main = factor * dot(d_low, qc[j, :, 0:512]) + dot(w_low, gr[j])
        rest = factor * dot(d_low, qc[j, :, 512:WIDE])
        part[s, :, :, 0:512] += main.reshape(2, 128, 512)
        part[s, :, :, 512:WIDE] += rest.reshape(2, 128, 128)

    def own(s, g, yy):
        rows = pl.ds(pl.multiple_of(yy * 32 + 16 * g, 16), 16)
        return part[s, 0, rows, :] + dsum[s, rows, :]

    def do_y1(s):
        c_d(s).wait_recv()
        for g in (0, 1):
            y1s[s, g, 0] = own(s, g, (y1, y3)[g])
            y1s[s, g, 1] = own(s, g, y2)
            c_y1(s, g).start()

    def do_y2(s):
        for g in (0, 1):
            c_y1(s, g).wait_recv()
            y2s[s, g] = own(s, g, (y3, y1)[g]) + y1r[s, g, 1]
            c_y2(s, g).start()

    def do_z(s):
        for g in (0, 1):
            c_y2(s, g).wait_recv()
            zs[s, 16 * g : 16 * g + 16, :] = own(s, g, y) + y1r[s, g, 0] + y2r[s, g]

        @pl.when(s > 0)
        def _():
            c_z(s).start()

    def each(act, last=3):
        def step(s, carry):
            act(s)
            return carry

        lax.fori_loop(0, jnp.minimum(zp, last) + 1, step, 0)

    def do_dq(j):
        for h in range(4):
            cols = pl.ds(h * 128, 128)
            m = mix[j, 0:512, cols]
            high = m.astype(BF16)
            rest = (m - high.astype(F32)).astype(BF16)
            got = dot(high, kw[:, cols], TN) + dot(rest, kw[:, cols], TN)
            dqs[j, :, cols] = factor * got
        for g in range(2):
            a = mix[j, 512:640, g * 256 : g * 256 + 128].T
            b = mix[j, 512:640, g * 256 + 128 : g * 256 + 256].T
            dqs[j, :, 512 + g * 128 : 640 + g * 128] = factor * jnp.concatenate(
                [a[:, 0:64], b[:, 0:64]], axis=1
            )

    def visit(t, carry):
        s, j = pick(ORDER_S, t), pick(ORDER_J, t)

        def arrive(k):
            @pl.when((t == {1: 1, 2: 4, 3: 12}[k]) & (zp >= k))
            def _():
                c_kzr(k).wait_recv()
                pass_on(k)

        arrive(1)
        arrive(2)
        arrive(3)

        @pl.when(((t < 2) | (t == 6) | (t == 12)) & (s <= zp))
        def _():
            c_kd(s).wait_recv()

        @pl.when(t == 2)
        def _():
            c_q(1).wait_recv()
            c_q(2).wait_recv()
            c_qh(0).start()
            c_qh(1).start()
            for k in (1, 2):
                c_st(k).wait_recv()
                project(k)

        @pl.when(t == 9)
        def _():
            c_qh(0).wait_recv()
            c_qh(1).wait_recv()
            c_st(3).wait_recv()
            project(3)

        @pl.when(t == 12)
        def _():
            each(lambda s: c_d(s).start(), 2)

        @pl.when(t == 14)
        def _():
            each(do_y1, 2)

        @pl.when(s <= zp)
        def _():
            tile(s, j)

        @pl.when(t == 12)
        def _():
            do_dq(3)
            c_dh(0).start()
            c_dh(1).start()

        return carry

    lax.fori_loop(0, 16, visit, 0)

    @pl.when(zp == 3)
    def _():
        c_d(3).start()

    for rel in (1, 0):
        half = c if rel == 0 else 1 - c
        for hh in (0, 1):
            cols = pl.ds(pl.multiple_of((2 * half + hh) * 128, 128), 128)
            got = jnp.zeros((512, 128), F32)
            for j in range(4):
                m = mix[j, 0:512, cols]
                high = m.astype(BF16)
                rest = (m - high.astype(F32)).astype(BF16)
                q = qb[j, :, cols]
                got = got + dot(jnp.concatenate([high, rest], axis=1), jnp.concatenate([q, q], axis=0))
            term[rel, :, :, :, hh * 128 : (hh + 1) * 128] = (factor * got).reshape(16, 4, 8, 128)
        if rel == 1:
            c_t.start()
    each(do_y2, 2)
    c_t.wait_recv()
    for j in range(4):
        turn = (x, x1, x3, x2)[j]
        got = (term[0, :, turn] + termr[:, turn]).reshape(128, 256)
        if j == 0:
            wx0[...] = got
        else:
            wxs[j] = got.astype(BF16)
            c_wx(j).start()

    do_dq(1)
    c_dh(1).wait_recv()
    dqs[1, 64:128, :] += dqh[1]
    c_dq(1).start()
    do_dq(2)
    c_dh(0).wait_recv()
    dqs[2, 0:64, :] += dqh[0]
    c_dq(2).start()

    @pl.when(zp == 3)
    def _():
        do_y1(3)

    each(do_z, 2)
    got = wx0[...]
    for j in (1, 2, 3):
        c_wx(j).wait_recv()
        got = got + wxr[j].astype(F32)
    wz[...] = got.reshape(16, 8, 256)

    def go(d, carry):
        c_wz(d).start()
        return carry

    lax.fori_loop(1, 16, go, 0)

    @pl.when(zp == 3)
    def _():
        do_y2(3)

    do_dq(0)

    @pl.when(zp == 3)
    def _():
        do_z(3)

    def wait_z(d, carry):
        c_zr(d).wait_recv()
        zs[0] += zr[d]
        return carry

    lax.fori_loop(1, more + 1, wait_z, 0)
    fin[0] = zs[0]
    for j in (1, 2, 3):
        c_f(j).start()

    def wait_wz(d, total):
        c_wz(d).wait_recv()
        return total + wzr[d]

    wf[...] = lax.fori_loop(1, 16, wait_wz, wz[z])
    c_wf.start()

    c_dq(1).wait_recv()
    c_dq(2).wait_recv()
    o_main[...] = dqs[0, :, 0:512] + dqr[0, :, 0:512] + dqr[1, :, 0:512]
    o_rot[...] = dqs[0, :, 512:768] + dqr[0, :, 512:768] + dqr[1, :, 512:768]

    for j in range(4):
        if j > 0:
            c_f(j).wait_recv()
        rows = pl.ds(pl.multiple_of((y, y1, y3, y2)[j] * 32, 32), 32)
        o_lat[rows, :] = fin[j, :, 0:512]
        o_krot[rows, :] = fin[j, :, 512:640]
    c_wf.wait_recv()

    @pl.when(c == 0)
    def _():
        o_weight[:, 0:256] = wf[0:4, :]
        o_weight[:, 256:512] = wfr[0:4, :]

    @pl.when(c == 1)
    def _():
        o_weight[:, 0:256] = wfr[4:8, :]
        o_weight[:, 256:512] = wf[4:8, :]

    def drain(s):
        @pl.when(more > 0)
        def _():
            c_kz(s).wait_send()

        c_kd(s).wait_send()
        c_d(s).wait_send()
        for g in (0, 1):
            c_y1(s, g).wait_send()
            c_y2(s, g).wait_send()

        @pl.when(s > 0)
        def _():
            c_z(s).wait_send()

    each(drain)
    c_t.wait_send()
    c_wf.wait_send()
    for i in (0, 1):
        c_q(1 + i).wait_send()
        c_qh(i).wait_send()
        c_dh(i).wait_send()
        c_dq(1 + i).wait_send()
    for j in (1, 2, 3):
        c_st(j).wait_send()
        c_wx(j).wait_send()
        c_f(j).wait_send()

    def drain_wz(d, carry):
        c_wz(d).wait_send()
        return carry

    lax.fori_loop(1, 16, drain_wz, 0)


def put_out(a, b, d, e, f, oa, ob, od, oe, of):
    oa[...] = a[...]
    ob[...] = b[...]
    od[...] = d[...]
    oe[...] = e[...].T[0:64, :]
    of[...] = f[...]


def per_device(query_main, query_rotary, latent, key_rotary, key_weight, value_weight, head_output, output_grad, row_logsum):
    v = pl.BlockSpec(memory_space=pltpu.VMEM)
    hbm = pl.BlockSpec(memory_space=pl.ANY)
    dma = pltpu.SemaphoreType.DMA
    scratch = [
        pltpu.VMEM((4, 128, 1280), BF16),
        pltpu.VMEM((4, 8, 512), F32),
        pltpu.VMEM((4, 512, WIDE), BF16),
        pltpu.VMEM((4, 512, 512), BF16),
        pltpu.VMEM((4, 2, 128, WIDE), BF16),
        pltpu.VMEM((4, WIDE, 512), F32),
        pltpu.VMEM((4, 2, 128, WIDE), F32),
        pltpu.VMEM((4, 128, WIDE), F32),
        pltpu.VMEM((4, 2, 2, 16, WIDE), F32),
        pltpu.VMEM((4, 2, 2, 16, WIDE), F32),
        pltpu.VMEM((4, 2, 16, WIDE), F32),
        pltpu.VMEM((4, 2, 16, WIDE), F32),
        pltpu.VMEM((4, 32, WIDE), F32),
        pltpu.VMEM((4, 32, WIDE), F32),
        pltpu.VMEM((4, 32, WIDE), F32),
        pltpu.VMEM((4, 128, 768), F32),
        pltpu.VMEM((2, 64, 768), F32),
        pltpu.VMEM((2, 128, 768), F32),
        pltpu.VMEM((2, 16, 4, 8, 256), F32),
        pltpu.VMEM((16, 4, 8, 256), F32),
        pltpu.VMEM((128, 256), F32),
        pltpu.VMEM((4, 128, 256), BF16),
        pltpu.VMEM((4, 128, 256), BF16),
        pltpu.VMEM((16, 8, 256), F32),
        pltpu.VMEM((16, 8, 256), F32),
        pltpu.VMEM((8, 256), F32),
        pltpu.VMEM((8, 256), F32),
        dma((4,)),
        dma((5,)), dma((5,)),
        dma((4,)), dma((4,)),
        dma((4,)), dma((5,)),
        dma((4,)), dma((4,)),
        dma((4,)), dma((4,)),
        dma((4, 2)), dma((4, 2)),
        dma((4, 2)), dma((4, 2)),
        dma((4,)), dma((4,)),
        dma((4,)), dma((4,)),
        dma((2,)), dma((2,)),
        dma((3,)), dma((3,)),
        dma, dma,
        dma((4,)), dma((4,)),
        dma((16,)), dma((16,)),
        dma, dma,
    ]
    got = pl.pallas_call(
        body,
        out_shape=(
            jax.ShapeDtypeStruct((128, 512), F32),
            jax.ShapeDtypeStruct((128, 256), F32),
            jax.ShapeDtypeStruct((128, 512), F32),
            jax.ShapeDtypeStruct((128, 128), F32),
            jax.ShapeDtypeStruct((4, 512), F32),
        ),
        in_specs=[hbm, hbm, hbm, v, v, v, v, hbm, v],
        out_specs=(v,) * 5,
        scratch_shapes=scratch,
        compiler_params=pltpu.CompilerParams(
            collective_id=0, has_side_effects=True, vmem_limit_bytes=56 * 1024 * 1024
        ),
    )(query_main, query_rotary, latent, key_rotary.T, key_weight, value_weight, head_output, output_grad, row_logsum)
    main, rot, lat, krot, weight = pl.pallas_call(
        put_out,
        out_shape=(
            jax.ShapeDtypeStruct((128, 512), F32),
            jax.ShapeDtypeStruct((128, 256), F32),
            jax.ShapeDtypeStruct((128, 512), F32),
            jax.ShapeDtypeStruct((64, 128), F32),
            jax.ShapeDtypeStruct((4, 512), F32),
        ),
        in_specs=[v] * 5,
        out_specs=(v,) * 5,
    )(*got)
    return main, rot, lat, krot.T, weight


def solution(mesh):
    finer = Mesh(mesh.devices.reshape(16, 4, 2, mesh.shape["tp"]), ("z", "x", "c", "y"))
    return jax.shard_map(
        per_device,
        mesh=finer,
        in_specs=(
            P(SP, "y"),
            P(SP, "y"),
            P(SP, None),
            P(SP, None),
            P(None, "y"),
            P(None, "y"),
            P(SP, "y"),
            P(SP, "y"),
            P("y", SP),
        ),
        out_specs=(P(SP, "y"), P(SP, "y"), P(SP, None), P(SP, None), P(SP, "y")),
        check_vma=False,
    )
```

```python
import jax
import jax.numpy as jnp
from jax import lax
from jax.experimental import pallas as pl
from jax.experimental.pallas import tpu as pltpu
from jax.sharding import Mesh
from jax.sharding import PartitionSpec as P

MESH = pl.DeviceIdType.MESH
SP = ("z", "x", "c")
F32 = jnp.float32
BF16 = jnp.bfloat16
WIDE = 640
NT = (((1,), (1,)), ((), ()))
TN = (((0,), (0,)), ((), ()))


def dot(a, b, dims=(((1,), (0,)), ((), ()))):
    return lax.dot_general(a, b, dims, preferred_element_type=F32)


def pick(table, t):
    out = jnp.int32(0)
    for k, v in enumerate(table):
        if v:
            out = out + jnp.where(t == k, v, 0)
    return out


def body(
    qm, qr, lat, krt, kwh, vwh, hoh, og, lsh,
    o_main, o_rot, o_lat, o_krot, o_weight,
    kw, vw, ho, ls, krv, qb, st, sts, qc, gr, keys, mix, part, dsum, y1s, y1r, y2s, y2r, zs, zr, fin,
    dqs, dqh, dqr, term, termr, wx0, wxs, wxr, wz, wzr, wf, wfr,
    s_loc, s_out, hop, s_q, r_q, s_st, r_st, s_kz, r_kz, s_kd, r_kd, s_d, r_d, s_y1, r_y1, s_y2, r_y2,
    s_z, r_z, s_f, r_f, s_dh, r_dh, s_dq, r_dq, s_t, r_t, s_wx, r_wx, s_wz, r_wz, s_wf, r_wf,
):
    z, x, c, y = (lax.axis_index(a) for a in ("z", "x", "c", "y"))
    factor = 192.0 ** (-0.5)
    zp = jnp.where(z < 3, z, (z + 1) % 4)
    planes = jnp.where(z < 3, 3, jnp.where(z < 15, 4, 1))
    more = planes - 1 - zp
    sib = {"c": 1 - c}
    x1, x3, x2 = x + 1 - 2 * (x % 2), 3 - x, (x + 2) % 4
    y1, y3, y2 = y + 1 - 2 * (y % 2), 3 - y, (y + 2) % 4
    xdev = (None, {"x": x1}, {"x": x3}, {"x": x2})
    ydev = (None, {"y": y1}, {"y": y3}, {"y": y2})

    def remote(src, dst, ss, rs, dev):
        return pltpu.make_async_remote_copy(
            src_ref=src, dst_ref=dst, send_sem=ss, recv_sem=rs, device_id=dev, device_id_type=MESH
        )

    def c_q(j, p):
        return remote(qb.at[0, p], qb.at[j, p], s_q.at[j, p], r_q.at[j, p], xdev[j])

    def c_qh(i, p):
        rows = pl.ds(64 * i, 64)
        return remote(qb.at[1 + i, p, rows], qb.at[3, p, rows], s_q.at[3 + i, p], r_q.at[3 + i, p], xdev[2 - i])

    def c_st(j):
        return remote(st.at[0], st.at[j], s_st.at[j], r_st.at[j], xdev[j])

    def c_kz(s):
        return remote(keys.at[s, 0], keys.at[s + 1, 0], s_kz.at[s], r_kz.at[s + 1], {"z": z + 1})

    def c_kzr(s):
        return remote(keys.at[s, 0], keys.at[s, 0], s_kz.at[s], r_kz.at[s], {"z": z - 1})

    def c_kd(s):
        return remote(keys.at[s, 0], keys.at[s, 1], s_kd.at[s], r_kd.at[s], sib)

    def c_d(s):
        return remote(part.at[s, 1], dsum.at[s], s_d.at[s], r_d.at[s], sib)

    def c_y1(s, g):
        return remote(y1s.at[s, g], y1r.at[s, g], s_y1.at[s, g], r_y1.at[s, g], ydev[1 + g])

    def c_y2(s, g):
        return remote(y2s.at[s, g], y2r.at[s, g], s_y2.at[s, g], r_y2.at[s, g], ydev[2 - g])

    def c_z(s):
        return remote(zs.at[s], zr.at[s], s_z.at[s], r_z.at[s], {"z": z - s})

    def c_zr(s):
        return remote(zs.at[s], zr.at[s], s_z.at[s], r_z.at[s], {"z": z + s})

    def c_f(j):
        return remote(fin.at[0], fin.at[j], s_f.at[j], r_f.at[j], ydev[j])

    def c_dh(i):
        rows = pl.ds(64 * i, 64)
        return remote(dqs.at[3, rows], dqh.at[i], s_dh.at[i], r_dh.at[i], xdev[1 + i])

    def c_dq(j):
        return remote(dqs.at[j], dqr.at[j - 1], s_dq.at[j], r_dq.at[j], xdev[j])

    c_t = remote(term.at[1], termr, s_t, r_t, sib)

    def c_wx(j):
        return remote(wxs.at[j], wxr.at[j], s_wx.at[j], r_wx.at[j], xdev[j])

    def c_wz(d):
        to = (z + d) % 16
        return remote(wz.at[to], wzr.at[d], s_wz.at[d], r_wz.at[d], {"z": to})

    c_wf = remote(wf, wfr, s_wf, r_wf, sib)

    barrier = pltpu.get_barrier_semaphore()
    for dev in (sib, *xdev[1:], *ydev[1:], *({"z": (z + d) % 16} for d in (1, 2, 3, 13, 14, 15))):
        pl.semaphore_signal(barrier, inc=1, device_id=dev, device_id_type=MESH)
    first = [
        (krt, krv),
        (lat, keys.at[0, 0, :, 0:512]),
        (qm.at[:, 0:256], qb.at[0, 0, :, 0:256]),
        (qr.at[:, 0:128], qb.at[0, 0, :, 256:384]),
        (og.at[:, 0:256], qb.at[0, 0, :, 384:640]),
        (qm.at[:, 256:512], qb.at[0, 1, :, 0:256]),
        (qr.at[:, 128:256], qb.at[0, 1, :, 256:384]),
        (og.at[:, 256:512], qb.at[0, 1, :, 384:640]),
        (kwh, kw),
        (vwh, vw),
        (hoh, ho),
        (lsh, ls),
    ]
    loads = [pltpu.make_async_copy(a, b, s_loc.at[i]) for i, (a, b) in enumerate(first)]
    for copy in loads:
        copy.start()
    loads[0].wait()
    keys[0, 0, :, 512:WIDE] = jnp.concatenate([krv[...].T, jnp.zeros((128, 64), BF16)], axis=1)
    for copy in loads[1:8]:
        copy.wait()
    pl.semaphore_wait(barrier, 13)

    def relay(i):
        for d in (3, 13):
            pl.semaphore_signal(hop.at[i], inc=1, device_id={"z": (z + d) % 16}, device_id_type=MESH)

    def pass_on(s):
        if s < 3:

            @pl.when(more > 0)
            def _():
                c_kz(s).start()

        c_kd(s).start()

    for p in (0, 1):
        c_q(1, p).start()
        c_q(2, p).start()
        if p == 0:
            pass_on(0)
    relay(0)

    def rows_of(slot):
        if slot in (0, 3):
            return [(slot, h) for h in range(4)]
        return [(j, 2 * (slot - 1) + h) for j in (1, 2) for h in (0, 1)]

    def place_of(j, h):
        if j in (0, 3):
            return j, h
        return 1 + h // 2, 2 * (j - 1) + h % 2

    for copy in loads[8:]:
        copy.wait()
    ones = jnp.ones((8, 128), F32)
    for h in range(4):
        cols = pl.ds(h * 128, 128)
        prod = ho[:, cols].astype(F32) * qb[0, h // 2, :, 384 + h % 2 * 128 : 512 + h % 2 * 128].astype(F32)
        sums = lax.dot_general(
            ones, prod, NT, precision=lax.Precision.HIGHEST, preferred_element_type=F32
        )
        st[0, 1:2, cols] = sums[0:1, :]
        st[0, 0:1, cols] = ls[h : h + 1, :]
    for j in (1, 2, 3):
        c_st(j).start()

    def project(slot):
        for b, (j, h) in enumerate(rows_of(slot)):
            p, k = h // 2, h % 2
            cols = pl.ds(h * 128, 128)
            rows = pl.ds(b * 128, 128)
            qc[slot, rows, 0:512] = dot(qb[j, p, :, k * 128 : k * 128 + 128], kw[:, cols], NT).astype(BF16)
            gr[slot, rows, :] = dot(qb[j, p, :, 384 + k * 128 : 512 + k * 128], vw[:, cols], NT).astype(BF16)
            rot = qb[j, p, :, 256 + k * 64 : 320 + k * 64]
            qc[slot, rows, 512:WIDE] = jnp.concatenate([rot, jnp.zeros((128, 64), BF16)], axis=1)
            sts[slot, 0:2, rows] = st[j, 0:2, cols]

    project(0)
    mix[...] = jnp.zeros_like(mix)
    part[...] = jnp.zeros_like(part)

    def tile(s, j):
        kt = keys[s].reshape(256, WIDE)
        turn_a = jnp.where(j == 0, x, jnp.where(j == 3, x2, x1))
        turn_b = jnp.where(j == 0, x, jnp.where(j == 3, x2, x3))
        far = jnp.where(s > 0, 1 << 20, 0)
        first = (2 * x + c) * 128 - far
        second = (2 * x + 1 - c) * 128 - 128 - far
        k_row = lax.broadcasted_iota(jnp.int32, (256, 1), 0)
        k_place = jnp.where(k_row < 128, k_row + first, k_row + second)
        q_col = lax.broadcasted_iota(jnp.int32, (1, 512), 1)
        q_place = q_col % 128 + jnp.where(q_col < 256, 2 * turn_a + c, 2 * turn_b + c) * 128
        scores = dot(kt, qc[j], NT)
        weights = jnp.where(k_place <= q_place, jnp.exp(factor * scores - sts[j, 0:1, :]), 0.0)
        slopes = dot(kt[:, 0:512], gr[j], NT)
        dscores = weights * (slopes - sts[j, 1:2, :])
        w_low = weights.astype(BF16)
        d_low = dscores.astype(BF16)
        mix[j] += dot(kt, d_low, TN)
        main = factor * dot(d_low, qc[j, :, 0:512]) + dot(w_low, gr[j])
        rest = factor * dot(d_low, qc[j, :, 512:WIDE])
        part[s, :, :, 0:512] += main.reshape(2, 128, 512)
        part[s, :, :, 512:WIDE] += rest.reshape(2, 128, 128)

    def own(s, g, yy):
        rows = pl.ds(pl.multiple_of(yy * 32 + 16 * g, 16), 16)
        return part[s, 0, rows, :] + dsum[s, rows, :]

    def do_y1(s):
        c_d(s).wait_recv()
        for g in (0, 1):
            y1s[s, g, 0] = own(s, g, (y1, y3)[g])
            y1s[s, g, 1] = own(s, g, y2)
            c_y1(s, g).start()

    def do_y2(s):
        for g in (0, 1):
            c_y1(s, g).wait_recv()
            y2s[s, g] = own(s, g, (y3, y1)[g]) + y1r[s, g, 1]
            c_y2(s, g).start()

    def do_z(s):
        for g in (0, 1):
            c_y2(s, g).wait_recv()
            zs[s, 16 * g : 16 * g + 16, :] = own(s, g, y) + y1r[s, g, 0] + y2r[s, g]

        if s > 0:
            c_z(s).start()

    def have(s, act):
        @pl.when(zp >= s)
        def _():
            act(s)

    def do_dq(j):
        for h in range(4):
            cols = pl.ds(h * 128, 128)
            slot, b = place_of(j, h)
            m = mix[slot, 0:512, b * 128 : b * 128 + 128]
            high = m.astype(BF16)
            rest = (m - high.astype(F32)).astype(BF16)
            got = dot(high, kw[:, cols], TN) + dot(rest, kw[:, cols], TN)
            dqs[j, :, cols] = factor * got
        for g in range(2):
            pair = []
            for h in (2 * g, 2 * g + 1):
                slot, b = place_of(j, h)
                pair.append(mix[slot, 512:640, b * 128 : b * 128 + 128].T[:, 0:64])
            dqs[j, :, 512 + g * 128 : 640 + g * 128] = factor * jnp.concatenate(pair, axis=1)

    def run(*pairs):
        def visit(t, carry):
            s = pick([a for a, _ in pairs], t)

            @pl.when(s <= zp)
            def _():
                tile(s, pick([b for _, b in pairs], t))

            return carry

        lax.fori_loop(0, len(pairs), visit, 0)

    def arrive(s):
        c_kzr(s).wait_recv()
        pass_on(s)

    def ready(s):
        c_kd(s).wait_recv()

    def halves(p):
        for j in (1, 2):
            c_q(j, p).wait_recv()
        for i in (0, 1):
            c_qh(i, p).start()

    def give(s):
        c_d(s).start()

    ready(0)
    run((0, 0))
    have(1, arrive)
    have(1, ready)
    run((1, 0))
    halves(0)
    for j in (1, 2):
        c_st(j).wait_recv()
    project(1)
    run((0, 1), (1, 1))
    pl.semaphore_wait(hop.at[0], 2)
    relay(1)
    have(2, arrive)
    halves(1)
    have(2, ready)
    project(2)
    run((2, 0), (0, 2), (1, 2), (2, 1))
    have(3, arrive)
    for i in (0, 1):
        c_qh(i, 0).wait_recv()
        c_qh(i, 1).wait_recv()
    c_st(3).wait_recv()
    project(3)
    have(3, ready)
    run((3, 0), (3, 1), (3, 2), (3, 3))
    have(3, give)
    run((2, 2), (2, 3))
    have(2, give)
    have(3, do_y1)
    run((1, 3))
    have(1, give)
    have(2, do_y1)
    run((0, 3))
    give(0)

    def do_term(rel):
        p = c if rel == 0 else 1 - c
        for k in (0, 1):
            got = jnp.zeros((512, 128), F32)
            wide = pl.ds(pl.multiple_of((2 * p + k) * 128, 128), 128)
            for j in range(4):
                if j in (0, 3):
                    m = mix[j, 0:512, wide]
                else:
                    m = mix[1 + p, 0:512, (2 * (j - 1) + k) * 128 : (2 * (j - 1) + k + 1) * 128]
                high = m.astype(BF16)
                rest = (m - high.astype(F32)).astype(BF16)
                q = qb[j, p, :, k * 128 : k * 128 + 128]
                got = got + dot(jnp.concatenate([high, rest], axis=1), jnp.concatenate([q, q], axis=0))
            term[rel, :, :, :, k * 128 : (k + 1) * 128] = (factor * got).reshape(16, 4, 8, 128)

    do_term(1)
    c_t.start()
    do_dq(3)
    c_dh(0).start()
    c_dh(1).start()
    have(3, do_y2)
    have(1, do_y1)
    do_term(0)
    have(2, do_y2)
    do_y1(0)
    c_t.wait_recv()
    for j in (1, 2, 3, 0):
        turn = (x, x1, x3, x2)[j]
        got = (term[0, :, turn] + termr[:, turn]).reshape(128, 256)
        if j == 0:
            wx0[...] = got
        else:
            wxs[j] = got.astype(BF16)
            c_wx(j).start()
    have(3, do_z)
    have(1, do_y2)
    do_dq(1)
    do_dq(2)
    have(2, do_z)
    do_y2(0)

    c_dh(1).wait_recv()
    dqs[1, 64:128, :] += dqh[1]
    c_dq(1).start()
    c_dh(0).wait_recv()
    dqs[2, 0:64, :] += dqh[0]
    c_dq(2).start()
    have(1, do_z)

    pl.semaphore_wait(hop.at[1], 2)
    got = wx0[...]
    for j in (1, 2, 3):
        c_wx(j).wait_recv()
        got = got + wxr[j].astype(F32)
    wz[...] = got.reshape(16, 8, 256)

    def go(d, carry):
        c_wz(d).start()
        return carry

    lax.fori_loop(1, 16, go, 0)
    do_z(0)
    do_dq(0)

    def wait_z(d, carry):
        c_zr(d).wait_recv()
        zs[0] += zr[d]
        return carry

    lax.fori_loop(1, more + 1, wait_z, 0)
    fin[0] = zs[0]
    for j in (1, 2, 3):
        c_f(j).start()

    c_dq(1).wait_recv()
    c_dq(2).wait_recv()
    dqs[0] += dqr[0] + dqr[1]
    outs = [
        pltpu.make_async_copy(dqs.at[0, :, 0:512], o_main, s_out.at[0]),
        pltpu.make_async_copy(dqs.at[0, :, 512:768], o_rot, s_out.at[1]),
    ]
    for copy in outs:
        copy.start()

    def wait_wz(d, total):
        c_wz(d).wait_recv()
        return total + wzr[d]

    wf[...] = lax.fori_loop(1, 16, wait_wz, wz[z])
    c_wf.start()
    for j in range(4):
        if j > 0:
            c_f(j).wait_recv()
        rows = pl.ds(pl.multiple_of((y, y1, y3, y2)[j] * 32, 32), 32)
        late = [
            pltpu.make_async_copy(fin.at[j, :, 0:512], o_lat.at[rows], s_out.at[2 + 2 * j]),
            pltpu.make_async_copy(fin.at[j, :, 512:640], o_krot.at[rows], s_out.at[3 + 2 * j]),
        ]
        for copy in late:
            copy.start()
        outs += late
    c_wf.wait_recv()

    @pl.when(c == 0)
    def _():
        o_weight[:, 0:256] = wf[0:4, :]
        o_weight[:, 256:512] = wfr[0:4, :]

    @pl.when(c == 1)
    def _():
        o_weight[:, 0:256] = wfr[4:8, :]
        o_weight[:, 256:512] = wf[4:8, :]

    for copy in outs:
        copy.wait()

    def drain(s):
        if s < 3:

            @pl.when(more > 0)
            def _():
                c_kz(s).wait_send()

        c_kd(s).wait_send()
        c_d(s).wait_send()
        for g in (0, 1):
            c_y1(s, g).wait_send()
            c_y2(s, g).wait_send()
        if s > 0:
            c_z(s).wait_send()

    for s in range(4):
        have(s, drain)
    c_t.wait_send()
    c_wf.wait_send()
    for i in (0, 1):
        for p in (0, 1):
            c_q(1 + i, p).wait_send()
            c_qh(i, p).wait_send()
        c_dh(i).wait_send()
        c_dq(1 + i).wait_send()
    for j in (1, 2, 3):
        c_st(j).wait_send()
        c_wx(j).wait_send()
        c_f(j).wait_send()

    def drain_wz(d, carry):
        c_wz(d).wait_send()
        return carry

    lax.fori_loop(1, 16, drain_wz, 0)


def put_out(a, b, d, e, f, oa, ob, od, oe, of):
    oa[...] = a[...]
    ob[...] = b[...]
    od[...] = d[...]
    oe[...] = e[...].T[0:64, :]
    of[...] = f[...]


def per_device(query_main, query_rotary, latent, key_rotary, key_weight, value_weight, head_output, output_grad, row_logsum):
    v = pl.BlockSpec(memory_space=pltpu.VMEM)
    hbm = pl.BlockSpec(memory_space=pl.ANY)
    dma = pltpu.SemaphoreType.DMA
    scratch = [
        pltpu.VMEM((512, 512), BF16),
        pltpu.VMEM((512, 512), BF16),
        pltpu.VMEM((128, 512), BF16),
        pltpu.VMEM((4, 128), F32),
        pltpu.VMEM((64, 128), BF16),
        pltpu.VMEM((4, 2, 128, 640), BF16),
        pltpu.VMEM((4, 8, 512), F32),
        pltpu.VMEM((4, 8, 512), F32),
        pltpu.VMEM((4, 512, WIDE), BF16),
        pltpu.VMEM((4, 512, 512), BF16),
        pltpu.VMEM((4, 2, 128, WIDE), BF16),
        pltpu.VMEM((4, WIDE, 512), F32),
        pltpu.VMEM((4, 2, 128, WIDE), F32),
        pltpu.VMEM((4, 128, WIDE), F32),
        pltpu.VMEM((4, 2, 2, 16, WIDE), F32),
        pltpu.VMEM((4, 2, 2, 16, WIDE), F32),
        pltpu.VMEM((4, 2, 16, WIDE), F32),
        pltpu.VMEM((4, 2, 16, WIDE), F32),
        pltpu.VMEM((4, 32, WIDE), F32),
        pltpu.VMEM((4, 32, WIDE), F32),
        pltpu.VMEM((4, 32, WIDE), F32),
        pltpu.VMEM((4, 128, 768), F32),
        pltpu.VMEM((2, 64, 768), F32),
        pltpu.VMEM((2, 128, 768), F32),
        pltpu.VMEM((2, 16, 4, 8, 256), F32),
        pltpu.VMEM((16, 4, 8, 256), F32),
        pltpu.VMEM((128, 256), F32),
        pltpu.VMEM((4, 128, 256), BF16),
        pltpu.VMEM((4, 128, 256), BF16),
        pltpu.VMEM((16, 8, 256), F32),
        pltpu.VMEM((16, 8, 256), F32),
        pltpu.VMEM((8, 256), F32),
        pltpu.VMEM((8, 256), F32),
        dma((12,)),
        dma((10,)),
        pltpu.SemaphoreType.REGULAR((2,)),
        dma((5, 2)), dma((5, 2)),
        dma((4,)), dma((4,)),
        dma((4,)), dma((5,)),
        dma((4,)), dma((4,)),
        dma((4,)), dma((4,)),
        dma((4, 2)), dma((4, 2)),
        dma((4, 2)), dma((4, 2)),
        dma((4,)), dma((4,)),
        dma((4,)), dma((4,)),
        dma((2,)), dma((2,)),
        dma((3,)), dma((3,)),
        dma, dma,
        dma((4,)), dma((4,)),
        dma((16,)), dma((16,)),
        dma, dma,
    ]
    got = pl.pallas_call(
        body,
        out_shape=(
            jax.ShapeDtypeStruct((128, 512), F32),
            jax.ShapeDtypeStruct((128, 256), F32),
            jax.ShapeDtypeStruct((128, 512), F32),
            jax.ShapeDtypeStruct((128, 128), F32),
            jax.ShapeDtypeStruct((4, 512), F32),
        ),
        in_specs=[hbm] * 9,
        out_specs=(hbm,) * 4 + (v,),
        scratch_shapes=scratch,
        compiler_params=pltpu.CompilerParams(
            collective_id=0, has_side_effects=True, vmem_limit_bytes=56 * 1024 * 1024
        ),
    )(query_main, query_rotary, latent, key_rotary.T, key_weight, value_weight, head_output, output_grad, row_logsum)
    main, rot, lat, krot, weight = pl.pallas_call(
        put_out,
        out_shape=(
            jax.ShapeDtypeStruct((128, 512), F32),
            jax.ShapeDtypeStruct((128, 256), F32),
            jax.ShapeDtypeStruct((128, 512), F32),
            jax.ShapeDtypeStruct((64, 128), F32),
            jax.ShapeDtypeStruct((4, 512), F32),
        ),
        in_specs=[v] * 5,
        out_specs=(v,) * 5,
    )(*got)
    return main, rot, lat, krot.T, weight


def solution(mesh):
    finer = Mesh(mesh.devices.reshape(16, 4, 2, mesh.shape["tp"]), ("z", "x", "c", "y"))
    return jax.shard_map(
        per_device,
        mesh=finer,
        in_specs=(
            P(SP, "y"),
            P(SP, "y"),
            P(SP, None),
            P(SP, None),
            P(None, "y"),
            P(None, "y"),
            P(SP, "y"),
            P(SP, "y"),
            P("y", SP),
        ),
        out_specs=(P(SP, "y"), P(SP, "y"), P(SP, None), P(SP, None), P(SP, "y")),
        check_vma=False,
    )
```

```python
import jax
import jax.numpy as jnp
from jax import lax
from jax.experimental import pallas as pl
from jax.experimental.pallas import tpu as pltpu
from jax.sharding import Mesh
from jax.sharding import PartitionSpec as P

MESH = pl.DeviceIdType.MESH
SP = ("z", "x", "c")
F32 = jnp.float32
BF16 = jnp.bfloat16
WIDE = 640
LOG2E = 1.4426950408889634
NT = (((1,), (1,)), ((), ()))
TN = (((0,), (0,)), ((), ()))


def dot(a, b, dims=(((1,), (0,)), ((), ()))):
    return lax.dot_general(a, b, dims, preferred_element_type=F32)


def pick(table, t):
    out = jnp.int32(0)
    for k, v in enumerate(table):
        if v:
            out = out + jnp.where(t == k, v, 0)
    return out


def body(
    qm, qr, lat, krt, kwh, vwh, hoh, og, lsh,
    o_main, o_rot, o_lat, o_krot, o_weight,
    krots, kw, vw, ho, ls, krv, qb, st, sts, qc, gr, keys, mix, part, dsum, y1s, y1r, y2s, y2r, zs, zr, fin,
    dqs, dqh, dqr, term, termr, wx0, wxs, wxr, wz, wzr, wf, wfr,
    s_loc, hop, s_q, r_q, s_st, r_st, s_kz, r_kz, s_kd, r_kd, s_d, r_d, s_y1, r_y1, s_y2, r_y2,
    s_z, r_z, s_f, r_f, s_dh, r_dh, s_dq, r_dq, s_t, r_t, s_wx, r_wx, s_wz, r_wz, s_wf, r_wf,
):
    z, x, c, y = (lax.axis_index(a) for a in ("z", "x", "c", "y"))
    factor = 192.0 ** (-0.5)
    zp = jnp.where(z < 3, z, (z + 1) % 4)
    planes = jnp.where(z < 3, 3, jnp.where(z < 15, 4, 1))
    more = planes - 1 - zp
    sib = {"c": 1 - c}
    x1, x3, x2 = x + 1 - 2 * (x % 2), 3 - x, (x + 2) % 4
    y1, y3, y2 = y + 1 - 2 * (y % 2), 3 - y, (y + 2) % 4
    xdev = (None, {"x": x1}, {"x": x3}, {"x": x2})
    ydev = (None, {"y": y1}, {"y": y3}, {"y": y2})

    def remote(src, dst, ss, rs, dev):
        return pltpu.make_async_remote_copy(
            src_ref=src, dst_ref=dst, send_sem=ss, recv_sem=rs, device_id=dev, device_id_type=MESH
        )

    def c_q(j, p):
        return remote(qb.at[0, p], qb.at[j, p], s_q.at[j, p], r_q.at[j, p], xdev[j])

    def c_qh(i, p):
        rows = pl.ds(64 * i, 64)
        return remote(qb.at[1 + i, p, rows], qb.at[3, p, rows], s_q.at[3 + i, p], r_q.at[3 + i, p], xdev[2 - i])

    def c_st(j):
        if j == 3:
            return remote(st.at[1], st.at[3], s_st.at[3], r_st.at[3], xdev[2])
        return remote(st.at[0], st.at[j], s_st.at[j], r_st.at[j], xdev[j])

    def c_kz(s):
        return remote(keys.at[s, 0], keys.at[s + 1, 0], s_kz.at[s], r_kz.at[s + 1], {"z": z + 1})

    def c_kzr(s):
        return remote(keys.at[s, 0], keys.at[s, 0], s_kz.at[s], r_kz.at[s], {"z": z - 1})

    def c_kd(s):
        return remote(keys.at[s, 0], keys.at[s, 1], s_kd.at[s], r_kd.at[s], sib)

    def c_d(s):
        return remote(part.at[s, 1], dsum.at[s], s_d.at[s], r_d.at[s], sib)

    def c_y1(s, g):
        return remote(y1s.at[s, g], y1r.at[s, g], s_y1.at[s, g], r_y1.at[s, g], ydev[1 + g])

    def c_y2(s, g):
        return remote(y2s.at[s, g], y2r.at[s, g], s_y2.at[s, g], r_y2.at[s, g], ydev[2 - g])

    def c_z(s):
        return remote(zs.at[s], zr.at[s], s_z.at[s], r_z.at[s], {"z": z - s})

    def c_zr(s):
        return remote(zs.at[s], zr.at[s], s_z.at[s], r_z.at[s], {"z": z + s})

    def c_f(j):
        return remote(fin.at[0], fin.at[j], s_f.at[j], r_f.at[j], ydev[j])

    def c_dh(i):
        rows = pl.ds(64 * i, 64)
        return remote(dqs.at[3, rows], dqh.at[i], s_dh.at[i], r_dh.at[i], xdev[1 + i])

    def c_dq(j):
        return remote(dqs.at[j], dqr.at[j - 1], s_dq.at[j], r_dq.at[j], xdev[j])

    c_t = remote(term.at[1], termr, s_t, r_t, sib)

    def c_wx(j):
        return remote(wxs.at[j], wxr.at[j], s_wx.at[j], r_wx.at[j], xdev[j])

    def c_wz(d):
        to = (z + d) % 16
        return remote(wz.at[to], wzr.at[d], s_wz.at[d], r_wz.at[d], {"z": to})

    c_wf = remote(wf, wfr, s_wf, r_wf, sib)

    barrier = pltpu.get_barrier_semaphore()
    for dev in (sib, *xdev[1:3], *ydev[1:3], {"z": (z + 1) % 16}, {"z": (z + 15) % 16}):
        pl.semaphore_signal(barrier, inc=1, device_id=dev, device_id_type=MESH)
    first = [
        (krt, krv),
        (lat, keys.at[0, 0, :, 0:512]),
        (qm.at[:, 0:256], qb.at[0, 0, :, 0:256]),
        (qr.at[:, 0:128], qb.at[0, 0, :, 256:384]),
        (og.at[:, 0:256], qb.at[0, 0, :, 384:640]),
        (qm.at[:, 256:512], qb.at[0, 1, :, 0:256]),
        (qr.at[:, 128:256], qb.at[0, 1, :, 256:384]),
        (og.at[:, 256:512], qb.at[0, 1, :, 384:640]),
        (kwh, kw),
        (vwh, vw),
        (hoh, ho),
        (lsh, ls),
    ]
    loads = [pltpu.make_async_copy(a, b, s_loc.at[i]) for i, (a, b) in enumerate(first)]
    for copy in loads:
        copy.start()
    loads[0].wait()
    keys[0, 0, :, 512:WIDE] = jnp.concatenate([krv[...].T, jnp.zeros((128, 64), BF16)], axis=1)
    for copy in loads[1:8]:
        copy.wait()
    pl.semaphore_wait(barrier, 7)

    def relay(i):
        for d in (1 << i, 16 - (1 << i)):
            pl.semaphore_signal(hop.at[i], inc=1, device_id={"z": (z + d) % 16}, device_id_type=MESH)
        if i == 0:
            for dev in (*xdev[1:3], *ydev[1:3]):
                pl.semaphore_signal(hop.at[i], inc=1, device_id=dev, device_id_type=MESH)

    def pass_on(s):
        if s < 3:

            @pl.when(more > 0)
            def _():
                c_kz(s).start()

        c_kd(s).start()

    c_q(1, 0).start()
    c_q(2, 0).start()
    pass_on(0)
    relay(0)

    def rows_of(slot):
        if slot in (0, 3):
            return [(slot, h) for h in range(4)]
        return [(j, 2 * (slot - 1) + h) for j in (1, 2) for h in (0, 1)]

    def place_of(j, h):
        if j in (0, 3):
            return j, h
        return 1 + h // 2, 2 * (j - 1) + h % 2

    for copy in loads[8:]:
        copy.wait()
    ones = jnp.ones((8, 128), F32)
    for h in range(4):
        cols = pl.ds(h * 128, 128)
        prod = ho[:, cols].astype(F32) * qb[0, h // 2, :, 384 + h % 2 * 128 : 512 + h % 2 * 128].astype(F32)
        sums = lax.dot_general(
            ones, prod, NT, precision=lax.Precision.HIGHEST, preferred_element_type=F32
        )
        st[0, 1:2, cols] = sums[0:1, :]
        st[0, 0:1, cols] = LOG2E * ls[h : h + 1, :]
    for j in (1, 2):
        c_st(j).start()

    def project(slot):
        for b, (j, h) in enumerate(rows_of(slot)):
            p, k = h // 2, h % 2
            cols = pl.ds(h * 128, 128)
            rows = pl.ds(b * 128, 128)
            qc[slot, rows, 0:512] = dot(qb[j, p, :, k * 128 : k * 128 + 128], kw[:, cols], NT).astype(BF16)
            gr[slot, rows, :] = dot(qb[j, p, :, 384 + k * 128 : 512 + k * 128], vw[:, cols], NT).astype(BF16)
            rot = qb[j, p, :, 256 + k * 64 : 320 + k * 64]
            qc[slot, rows, 512:WIDE] = jnp.concatenate([rot, jnp.zeros((128, 64), BF16)], axis=1)
            sts[slot, 0:2, rows] = st[j, 0:2, cols]

    project(0)
    mix[...] = jnp.zeros_like(mix)
    part[...] = jnp.zeros_like(part)

    def tile(s, j):
        kt = keys[s].reshape(256, WIDE)
        turn_a = jnp.where(j == 0, x, jnp.where(j == 3, x2, x1))
        turn_b = jnp.where(j == 0, x, jnp.where(j == 3, x2, x3))
        far = jnp.where(s > 0, 1 << 20, 0)
        first = (2 * x + c) * 128 - far
        second = (2 * x + 1 - c) * 128 - 128 - far
        k_row = lax.broadcasted_iota(jnp.int32, (256, 1), 0)
        k_place = jnp.where(k_row < 128, k_row + first, k_row + second)
        q_col = lax.broadcasted_iota(jnp.int32, (1, 512), 1)
        q_place = q_col % 128 + jnp.where(q_col < 256, 2 * turn_a + c, 2 * turn_b + c) * 128
        scores = dot(kt, qc[j], NT)
        weights = jnp.where(
            k_place <= q_place, jnp.exp2((factor * LOG2E) * scores - sts[j, 0:1, :]), 0.0
        )
        slopes = dot(kt[:, 0:512], gr[j], NT)
        dscores = weights * (slopes - sts[j, 1:2, :])
        w_low = weights.astype(BF16)
        d_low = dscores.astype(BF16)
        mix[j] += dot(kt, d_low, TN)
        main = factor * dot(d_low, qc[j, :, 0:512]) + dot(w_low, gr[j])
        rest = factor * dot(d_low, qc[j, :, 512:WIDE])
        part[s, :, :, 0:512] += main.reshape(2, 128, 512)
        part[s, :, :, 512:WIDE] += rest.reshape(2, 128, 128)

    def own(s, g, yy):
        rows = pl.ds(pl.multiple_of(yy * 32 + 16 * g, 16), 16)
        return part[s, 0, rows, :] + dsum[s, rows, :]

    def do_y1(s):
        c_d(s).wait_recv()
        for g in (0, 1):
            y1s[s, g, 0] = own(s, g, (y1, y3)[g]).astype(BF16)
            y1s[s, g, 1] = own(s, g, y2).astype(BF16)
            c_y1(s, g).start()

    def do_y2(s):
        for g in (0, 1):
            c_y1(s, g).wait_recv()
            y2s[s, g] = own(s, g, (y3, y1)[g]) + y1r[s, g, 1].astype(F32)
            c_y2(s, g).start()

    def do_z(s):
        for g in (0, 1):
            c_y2(s, g).wait_recv()
            zs[s, 16 * g : 16 * g + 16, :] = own(s, g, y) + y1r[s, g, 0].astype(F32) + y2r[s, g]

        if s > 0:
            c_z(s).start()

    def have(s, act):
        @pl.when(zp >= s)
        def _():
            act(s)

    def do_dq(j):
        for h in range(4):
            cols = pl.ds(h * 128, 128)
            slot, b = place_of(j, h)
            m = mix[slot, 0:512, b * 128 : b * 128 + 128]
            high = m.astype(BF16)
            rest = (m - high.astype(F32)).astype(BF16)
            got = dot(high, kw[:, cols], TN) + dot(rest, kw[:, cols], TN)
            dqs[j, :, cols] = factor * got
        for g in range(2):
            pair = []
            for h in (2 * g, 2 * g + 1):
                slot, b = place_of(j, h)
                pair.append(mix[slot, 512:640, b * 128 : b * 128 + 128].T[:, 0:64])
            dqs[j, :, 512 + g * 128 : 640 + g * 128] = factor * jnp.concatenate(pair, axis=1)

    def run(*pairs):
        def visit(t, carry):
            s = pick([a for a, _ in pairs], t)

            @pl.when(s <= zp)
            def _():
                tile(s, pick([b for _, b in pairs], t))

            return carry

        lax.fori_loop(0, len(pairs), visit, 0)

    def arrive(s):
        c_kzr(s).wait_recv()
        pass_on(s)

    def ready(s):
        c_kd(s).wait_recv()

    def halves(p):
        for j in (1, 2):
            c_q(j, p).wait_recv()
        for i in (0, 1):
            c_qh(i, p).start()

    def give(s):
        c_d(s).start()

    ready(0)
    run((0, 0))
    pl.semaphore_wait(hop.at[0], 6)
    relay(1)
    have(1, arrive)
    c_q(1, 1).start()
    c_q(2, 1).start()
    have(1, ready)
    run((1, 0))
    halves(0)
    for j in (1, 2):
        c_st(j).wait_recv()
    c_st(3).start()
    project(1)
    run((0, 1), (1, 1))
    pl.semaphore_wait(hop.at[1], 2)
    relay(2)
    halves(1)
    project(2)
    run((0, 2))
    have(2, arrive)
    run((1, 2))
    have(2, ready)
    run((2, 0), (2, 1), (2, 2))
    for i in (0, 1):
        c_qh(i, 0).wait_recv()
        c_qh(i, 1).wait_recv()
    c_st(3).wait_recv()
    project(3)
    have(3, arrive)
    run((2, 3))
    have(2, give)
    run((1, 3))
    have(1, give)
    run((0, 3))
    give(0)
    have(2, do_y1)
    have(3, ready)
    run((3, 3))
    do_dq(3)
    c_dh(0).start()
    c_dh(1).start()
    have(1, do_y1)
    run((3, 1))
    do_y1(0)
    run((3, 2))
    have(2, do_y2)

    def do_term(rel, slots):
        p = c if rel == 0 else 1 - c
        for k in (0, 1):
            got = jnp.zeros((512, 128), F32)
            wide = pl.ds(pl.multiple_of((2 * p + k) * 128, 128), 128)
            for j in slots:
                if j in (0, 3):
                    m = mix[j, 0:512, wide]
                else:
                    m = mix[1 + p, 0:512, (2 * (j - 1) + k) * 128 : (2 * (j - 1) + k + 1) * 128]
                high = m.astype(BF16)
                rest = (m - high.astype(F32)).astype(BF16)
                q = qb[j, p, :, k * 128 : k * 128 + 128]
                got = got + dot(jnp.concatenate([high, rest], axis=1), jnp.concatenate([q, q], axis=0))
            got = (factor * got).reshape(16, 4, 8, 128)
            if len(slots) == 1:
                got = got + term[rel, :, :, :, k * 128 : (k + 1) * 128]
            term[rel, :, :, :, k * 128 : (k + 1) * 128] = got

    do_term(1, (1, 2, 3))
    do_term(0, (1, 2, 3))
    run((3, 0))
    have(3, give)
    do_term(1, (0,))
    c_t.start()
    do_term(0, (0,))
    have(1, do_y2)
    have(3, do_y1)
    do_y2(0)
    c_t.wait_recv()
    for j in (3, 1, 2, 0):
        turn = (x, x1, x3, x2)[j]
        got = (term[0, :, turn] + termr[:, turn]).reshape(128, 256)
        if j == 0:
            wx0[...] = got
        else:
            wxs[j] = got.astype(BF16)
            c_wx(j).start()
    have(2, do_z)

    do_dq(1)
    c_dh(1).wait_recv()
    dqs[1, 64:128, :] += dqh[1]
    c_dq(1).start()
    do_dq(2)
    c_dh(0).wait_recv()
    dqs[2, 0:64, :] += dqh[0]
    c_dq(2).start()
    have(3, do_y2)
    have(1, do_z)
    do_z(0)
    do_dq(0)

    pl.semaphore_wait(hop.at[2], 2)
    got = wx0[...]
    for j in (1, 2, 3):
        c_wx(j).wait_recv()
        got = got + wxr[j].astype(F32)
    wz[...] = got.reshape(16, 8, 256)

    def go(d, carry):
        c_wz(d).start()
        return carry

    lax.fori_loop(1, 16, go, 0)
    have(3, do_z)

    def wait_z(d, carry):
        c_zr(d).wait_recv()
        zs[0] += zr[d]
        return carry

    lax.fori_loop(1, more + 1, wait_z, 0)
    fin[0] = zs[0].astype(BF16)
    for j in (1, 2, 3):
        c_f(j).start()

    c_dq(1).wait_recv()
    c_dq(2).wait_recv()
    o_main[...] = dqs[0, :, 0:512] + dqr[0, :, 0:512] + dqr[1, :, 0:512]
    o_rot[...] = dqs[0, :, 512:768] + dqr[0, :, 512:768] + dqr[1, :, 512:768]

    def wait_wz(d, total):
        c_wz(d).wait_recv()
        return total + wzr[d]

    wf[...] = lax.fori_loop(1, 16, wait_wz, wz[z])
    c_wf.start()
    for j in range(4):
        if j > 0:
            c_f(j).wait_recv()
        rows = pl.ds(pl.multiple_of((y, y1, y3, y2)[j] * 32, 32), 32)
        got = zs[0] if j == 0 else fin[j].astype(F32)
        o_lat[rows, :] = got[:, 0:512]
        krots[rows, :] = got[:, 512:640]
    o_krot[...] = krots[...].T[0:64, :]
    c_wf.wait_recv()

    @pl.when(c == 0)
    def _():
        o_weight[:, 0:256] = wf[0:4, :]
        o_weight[:, 256:512] = wfr[0:4, :]

    @pl.when(c == 1)
    def _():
        o_weight[:, 0:256] = wfr[4:8, :]
        o_weight[:, 256:512] = wf[4:8, :]

    def drain(s):
        if s < 3:

            @pl.when(more > 0)
            def _():
                c_kz(s).wait_send()

        c_kd(s).wait_send()
        c_d(s).wait_send()
        for g in (0, 1):
            c_y1(s, g).wait_send()
            c_y2(s, g).wait_send()
        if s > 0:
            c_z(s).wait_send()

    for s in range(4):
        have(s, drain)
    c_t.wait_send()
    c_wf.wait_send()
    for i in (0, 1):
        for p in (0, 1):
            c_q(1 + i, p).wait_send()
            c_qh(i, p).wait_send()
        c_dh(i).wait_send()
        c_dq(1 + i).wait_send()
    for j in (1, 2, 3):
        c_st(j).wait_send()
        c_wx(j).wait_send()
        c_f(j).wait_send()

    def drain_wz(d, carry):
        c_wz(d).wait_send()
        return carry

    lax.fori_loop(1, 16, drain_wz, 0)


def put_out(*refs):
    ends, sems = refs[5:10], refs[10]
    copies = [pltpu.make_async_copy(a, b, sems.at[i]) for i, (a, b) in enumerate(zip(refs[:5], ends))]
    for copy in copies:
        copy.start()
    for copy in copies:
        copy.wait()


def per_device(query_main, query_rotary, latent, key_rotary, key_weight, value_weight, head_output, output_grad, row_logsum):
    v = pl.BlockSpec(memory_space=pltpu.VMEM)
    hbm = pl.BlockSpec(memory_space=pl.ANY)
    dma = pltpu.SemaphoreType.DMA
    scratch = [
        pltpu.VMEM((128, 128), F32),
        pltpu.VMEM((512, 512), BF16),
        pltpu.VMEM((512, 512), BF16),
        pltpu.VMEM((128, 512), BF16),
        pltpu.VMEM((4, 128), F32),
        pltpu.VMEM((64, 128), BF16),
        pltpu.VMEM((4, 2, 128, 640), BF16),
        pltpu.VMEM((4, 8, 512), F32),
        pltpu.VMEM((4, 8, 512), F32),
        pltpu.VMEM((4, 512, WIDE), BF16),
        pltpu.VMEM((4, 512, 512), BF16),
        pltpu.VMEM((4, 2, 128, WIDE), BF16),
        pltpu.VMEM((4, WIDE, 512), F32),
        pltpu.VMEM((4, 2, 128, WIDE), F32),
        pltpu.VMEM((4, 128, WIDE), F32),
        pltpu.VMEM((4, 2, 2, 16, WIDE), BF16),
        pltpu.VMEM((4, 2, 2, 16, WIDE), BF16),
        pltpu.VMEM((4, 2, 16, WIDE), F32),
        pltpu.VMEM((4, 2, 16, WIDE), F32),
        pltpu.VMEM((4, 32, WIDE), F32),
        pltpu.VMEM((4, 32, WIDE), F32),
        pltpu.VMEM((4, 32, WIDE), BF16),
        pltpu.VMEM((4, 128, 768), F32),
        pltpu.VMEM((2, 64, 768), F32),
        pltpu.VMEM((2, 128, 768), F32),
        pltpu.VMEM((2, 16, 4, 8, 256), F32),
        pltpu.VMEM((16, 4, 8, 256), F32),
        pltpu.VMEM((128, 256), F32),
        pltpu.VMEM((4, 128, 256), BF16),
        pltpu.VMEM((4, 128, 256), BF16),
        pltpu.VMEM((16, 8, 256), F32),
        pltpu.VMEM((16, 8, 256), F32),
        pltpu.VMEM((8, 256), F32),
        pltpu.VMEM((8, 256), F32),
        dma((12,)),
        pltpu.SemaphoreType.REGULAR((3,)),
        dma((5, 2)), dma((5, 2)),
        dma((4,)), dma((4,)),
        dma((4,)), dma((5,)),
        dma((4,)), dma((4,)),
        dma((4,)), dma((4,)),
        dma((4, 2)), dma((4, 2)),
        dma((4, 2)), dma((4, 2)),
        dma((4,)), dma((4,)),
        dma((4,)), dma((4,)),
        dma((2,)), dma((2,)),
        dma((3,)), dma((3,)),
        dma, dma,
        dma((4,)), dma((4,)),
        dma((16,)), dma((16,)),
        dma, dma,
    ]
    got = pl.pallas_call(
        body,
        out_shape=(
            pltpu.VMEM((128, 512), F32),
            pltpu.VMEM((128, 256), F32),
            pltpu.VMEM((128, 512), F32),
            pltpu.VMEM((64, 128), F32),
            pltpu.VMEM((4, 512), F32),
        ),
        in_specs=[hbm] * 9,
        out_specs=(v,) * 5,
        scratch_shapes=scratch,
        compiler_params=pltpu.CompilerParams(
            collective_id=0, has_side_effects=True, vmem_limit_bytes=56 * 1024 * 1024
        ),
    )(query_main, query_rotary, latent, key_rotary.T, key_weight, value_weight, head_output, output_grad, row_logsum)
    main, rot, lat, krot, weight = pl.pallas_call(
        put_out,
        out_shape=(
            jax.ShapeDtypeStruct((128, 512), F32),
            jax.ShapeDtypeStruct((128, 256), F32),
            jax.ShapeDtypeStruct((128, 512), F32),
            jax.ShapeDtypeStruct((64, 128), F32),
            jax.ShapeDtypeStruct((4, 512), F32),
        ),
        in_specs=[v] * 5,
        out_specs=(hbm,) * 5,
        scratch_shapes=[dma((5,))],
    )(*(pltpu.with_memory_space_constraint(a, pltpu.VMEM) for a in got))
    return main, rot, lat, krot.T, weight


def solution(mesh):
    finer = Mesh(mesh.devices.reshape(16, 4, 2, mesh.shape["tp"]), ("z", "x", "c", "y"))
    return jax.shard_map(
        per_device,
        mesh=finer,
        in_specs=(
            P(SP, "y"),
            P(SP, "y"),
            P(SP, None),
            P(SP, None),
            P(None, "y"),
            P(None, "y"),
            P(SP, "y"),
            P(SP, "y"),
            P("y", SP),
        ),
        out_specs=(P(SP, "y"), P(SP, "y"), P(SP, None), P(SP, None), P(SP, "y")),
        check_vma=False,
    )
```

```python
import jax
import jax.numpy as jnp
from jax import lax
from jax.experimental import pallas as pl
from jax.experimental.pallas import tpu as pltpu
from jax.sharding import Mesh
from jax.sharding import PartitionSpec as P

MESH = pl.DeviceIdType.MESH
SP = ("z", "x", "c")
F32 = jnp.float32
BF16 = jnp.bfloat16
WIDE = 640
LOG2E = 1.4426950408889634
NT = (((1,), (1,)), ((), ()))
TN = (((0,), (0,)), ((), ()))


def dot(a, b, dims=(((1,), (0,)), ((), ()))):
    return lax.dot_general(a, b, dims, preferred_element_type=F32)


def pick(table, t):
    out = jnp.int32(0)
    for k, v in enumerate(table):
        if v:
            out = out + jnp.where(t == k, v, 0)
    return out


def body(
    qm, qr, lat, krt, kwh, vwh, hoh, og, lsh,
    o_main, o_rot, o_lat, o_krot, o_weight,
    krots, kv, ho, ls, krv, qb, st, sts, qc, gr, keys, mix, part, dsum, y1s, y1r, y2s, y2r, zs, zr, fin,
    dqs, dqh, dqr, term, termr, wx0, wxs, wxr, wz, wzr,
    s_loc, hop, s_q, r_q, s_st, r_st, s_kz, r_kz, s_kd, r_kd, s_d, r_d, s_y1, r_y1, s_y2, r_y2,
    s_z, r_z, s_f, r_f, s_dh, r_dh, s_dq, r_dq, s_t, r_t, s_wx, r_wx, s_wz, r_wz,
):
    z, x, c, y = (lax.axis_index(a) for a in ("z", "x", "c", "y"))
    factor = 192.0 ** (-0.5)
    zp = jnp.where(z < 3, z, (z + 1) % 4)
    planes = jnp.where(z < 3, 3, jnp.where(z < 15, 4, 1))
    more = planes - 1 - zp
    sib = {"c": 1 - c}
    x1, x3, x2 = x + 1 - 2 * (x % 2), 3 - x, (x + 2) % 4
    y1, y3, y2 = y + 1 - 2 * (y % 2), 3 - y, (y + 2) % 4
    xdev = (None, {"x": x1}, {"x": x3}, {"x": x2})
    ydev = (None, {"y": y1}, {"y": y3}, {"y": y2})

    def remote(src, dst, ss, rs, dev):
        return pltpu.make_async_remote_copy(
            src_ref=src, dst_ref=dst, send_sem=ss, recv_sem=rs, device_id=dev, device_id_type=MESH
        )

    def c_q(j, p):
        return remote(qb.at[0, p], qb.at[j, p], s_q.at[0], r_q.at[p], xdev[j])

    def c_qh(i, p):
        rows = pl.ds(64 * i, 64)
        return remote(qb.at[1 + i, p, rows], qb.at[3, p, rows], s_q.at[1], r_q.at[2], xdev[2 - i])

    def c_st(j):
        if j == 3:
            return remote(st.at[1], st.at[3], s_st.at[1], r_st.at[1], xdev[2])
        return remote(st.at[0], st.at[j], s_st.at[0], r_st.at[0], xdev[j])

    def c_kz(s):
        return remote(keys.at[s, 0], keys.at[s + 1, 0], s_kz.at[s], r_kz.at[s], {"z": z + 1})

    def c_kzr(s):
        return remote(keys.at[s - 1, 0], keys.at[s, 0], s_kz.at[s - 1], r_kz.at[s - 1], {"z": z - 1})

    def c_kd(s):
        return remote(keys.at[s, 0], keys.at[s, 1], s_kd.at[s], r_kd.at[s], sib)

    def c_d(s):
        return remote(part.at[s, 1], dsum.at[s], s_d.at[s], r_d.at[s], sib)

    def c_y1(s, g):
        return remote(y1s.at[s, g], y1r.at[s, g], s_y1.at[s], r_y1.at[s], ydev[1 + g])

    def c_y2(s, g):
        return remote(y2s.at[s, g], y2r.at[s, g], s_y2.at[s], r_y2.at[s], ydev[2 - g])

    def c_z(s):
        return remote(zs.at[s], zr.at[s], s_z.at[s - 1], r_z.at[s - 1], {"z": z - s})

    def c_zr(s):
        return remote(zs.at[s], zr.at[s], s_z.at[s - 1], r_z.at[s - 1], {"z": z + s})

    def c_f(j):
        return remote(fin.at[0], fin.at[j], s_f.at[0], r_f.at[0], ydev[j])

    def c_dh(i):
        rows = pl.ds(64 * i, 64)
        return remote(dqs.at[3, rows], dqh.at[i], s_dh.at[0], r_dh.at[i], xdev[1 + i])

    def c_dq(j):
        return remote(dqs.at[j], dqr.at[j - 1], s_dq.at[0], r_dq.at[0], xdev[j])

    def c_t(j):
        turn = (x, x1, x3, x2)[j]
        return remote(term.at[1, :, turn], termr.at[:, turn], s_t.at[0], r_t.at[j], sib)

    def c_wx(j):
        return remote(wxs.at[j], wxr.at[j], s_wx.at[0], r_wx.at[0], xdev[j])

    def c_wz(k, d):
        to = (z + d) % 16
        own = c if k == 0 else 1 - c
        dev = {"z": to, "c": own}
        return remote(wz.at[own * 16 + to], wzr.at[16 * k + d], s_wz.at[0], r_wz.at[0], dev)

    def w_all(ref, sem):
        pltpu.make_async_copy(ref, ref, sem).wait()

    barrier = pltpu.get_barrier_semaphore()
    for dev in (sib, *xdev[1:3], *ydev[1:3], {"z": (z + 1) % 16}, {"z": (z + 15) % 16}):
        pl.semaphore_signal(barrier, inc=1, device_id=dev, device_id_type=MESH)
    first = [
        (krt, krv, 0),
        (lat, keys.at[0, 0, :, 0:512], 1),
        (qm.at[:, 0:256], qb.at[0, 0, :, 0:256], 2),
        (qr.at[:, 0:128], qb.at[0, 0, :, 256:384], 2),
        (og.at[:, 0:256], qb.at[0, 0, :, 384:640], 2),
        (qm.at[:, 256:512], qb.at[0, 1, :, 0:256], 2),
        (qr.at[:, 128:256], qb.at[0, 1, :, 256:384], 2),
        (og.at[:, 256:512], qb.at[0, 1, :, 384:640], 2),
        (kwh, kv.at[0], 3),
        (vwh, kv.at[1], 3),
        (hoh, ho, 4),
        (lsh, ls, 5),
    ]
    kw, vw = kv.at[0], kv.at[1]
    loads = [pltpu.make_async_copy(a, b, s_loc.at[i]) for a, b, i in first]
    for copy in loads:
        copy.start()
    loads[0].wait()
    keys[0, 0, :, 512:WIDE] = jnp.concatenate([krv[...].T, jnp.zeros((128, 64), BF16)], axis=1)
    loads[1].wait()
    w_all(qb.at[0], s_loc.at[2])
    pl.semaphore_wait(barrier, 7)

    def relay(i):
        for d in (1 << i, 16 - (1 << i)):
            pl.semaphore_signal(hop.at[i], inc=1, device_id={"z": (z + d) % 16}, device_id_type=MESH)
        if i == 0:
            for dev in (*xdev[1:3], *ydev[1:3]):
                pl.semaphore_signal(hop.at[i], inc=1, device_id=dev, device_id_type=MESH)

    def pass_on(s):
        if s < 3:

            @pl.when(more > 0)
            def _():
                c_kz(s).start()

        c_kd(s).start()

    c_q(1, 0).start()
    c_q(2, 0).start()
    pass_on(0)
    relay(0)

    def rows_of(slot):
        if slot in (0, 3):
            return [(slot, h) for h in range(4)]
        return [(j, 2 * (slot - 1) + h) for j in (1, 2) for h in (0, 1)]

    def place_of(j, h):
        if j in (0, 3):
            return j, h
        return 1 + h // 2, 2 * (j - 1) + h % 2

    w_all(kv, s_loc.at[3])
    for copy in loads[10:]:
        copy.wait()
    ones = jnp.ones((8, 128), F32)
    for h in range(4):
        cols = pl.ds(h * 128, 128)
        prod = ho[:, cols].astype(F32) * qb[0, h // 2, :, 384 + h % 2 * 128 : 512 + h % 2 * 128].astype(F32)
        sums = lax.dot_general(
            ones, prod, NT, precision=lax.Precision.HIGHEST, preferred_element_type=F32
        )
        st[0, 1:2, cols] = sums[0:1, :]
        st[0, 0:1, cols] = LOG2E * ls[h : h + 1, :]
    for j in (1, 2):
        c_st(j).start()

    def project(slot):
        for b, (j, h) in enumerate(rows_of(slot)):
            p, k = h // 2, h % 2
            cols = pl.ds(h * 128, 128)
            rows = pl.ds(b * 128, 128)
            qc[slot, rows, 0:512] = dot(qb[j, p, :, k * 128 : k * 128 + 128], kw[:, cols], NT).astype(BF16)
            gr[slot, rows, :] = dot(qb[j, p, :, 384 + k * 128 : 512 + k * 128], vw[:, cols], NT).astype(BF16)
            rot = qb[j, p, :, 256 + k * 64 : 320 + k * 64]
            qc[slot, rows, 512:WIDE] = jnp.concatenate([rot, jnp.zeros((128, 64), BF16)], axis=1)
            sts[slot, 0:2, rows] = st[j, 0:2, cols]

    project(0)
    mix[...] = jnp.zeros_like(mix)
    part[...] = jnp.zeros_like(part)

    def tile(s, j, masked):
        kt = keys[s].reshape(256, WIDE)
        turn_a = jnp.where(j == 0, x, jnp.where(j == 3, x2, x1))
        turn_b = jnp.where(j == 0, x, jnp.where(j == 3, x2, x3))
        far = jnp.where(s > 0, 1 << 20, 0)
        first = (2 * x + c) * 128 - far
        second = (2 * x + 1 - c) * 128 - 128 - far
        k_row = lax.broadcasted_iota(jnp.int32, (256, 1), 0)
        k_place = jnp.where(k_row < 128, k_row + first, k_row + second)
        q_col = lax.broadcasted_iota(jnp.int32, (1, 512), 1)
        q_place = q_col % 128 + jnp.where(q_col < 256, 2 * turn_a + c, 2 * turn_b + c) * 128
        scores = dot(kt, qc[j], NT)
        weights = jnp.exp2((factor * LOG2E) * scores - sts[j, 0:1, :])
        if masked:
            weights = jnp.where(k_place <= q_place, weights, 0.0)
        slopes = dot(kt[:, 0:512], gr[j], NT)
        dscores = weights * (slopes - sts[j, 1:2, :])
        w_low = weights.astype(BF16)
        d_low = dscores.astype(BF16)
        mix[j, 0:576, :] += dot(kt[:, 0:576], d_low, TN)
        main = factor * dot(d_low, qc[j, :, 0:512]) + dot(w_low, gr[j])
        rest = factor * dot(d_low, qc[j, :, 512:WIDE])
        part[s, :, :, 0:512] += main.reshape(2, 128, 512)
        part[s, :, :, 512:WIDE] += rest.reshape(2, 128, 128)

    def own(s, g, yy):
        rows = pl.ds(pl.multiple_of(yy * 32 + 16 * g, 16), 16)
        return part[s, 0, rows, :] + dsum[s, rows, :]

    def do_y1(s):
        c_d(s).wait_recv()
        for g in (0, 1):
            y1s[s, g, 0] = own(s, g, (y1, y3)[g]).astype(BF16)
            y1s[s, g, 1] = own(s, g, y2).astype(BF16)
            c_y1(s, g).start()

    def do_y2(s):
        w_all(y1r.at[s], r_y1.at[s])
        for g in (0, 1):
            y2s[s, g] = own(s, g, (y3, y1)[g]) + y1r[s, g, 1].astype(F32)
            c_y2(s, g).start()

    def do_z(s):
        w_all(y2r.at[s], r_y2.at[s])
        for g in (0, 1):
            zs[s, 16 * g : 16 * g + 16, :] = own(s, g, y) + y1r[s, g, 0].astype(F32) + y2r[s, g]
        if s > 0:
            c_z(s).start()

    def have(s, act):
        @pl.when(zp >= s)
        def _():
            act(s)

    def do_dq(j):
        for h in range(4):
            cols = pl.ds(h * 128, 128)
            slot, b = place_of(j, h)
            m = mix[slot, 0:512, b * 128 : b * 128 + 128]
            high = m.astype(BF16)
            rest = (m - high.astype(F32)).astype(BF16)
            got = dot(high, kw[:, cols], TN) + dot(rest, kw[:, cols], TN)
            dqs[j, :, cols] = factor * got
        for g in range(2):
            pair = []
            for h in (2 * g, 2 * g + 1):
                slot, b = place_of(j, h)
                pair.append(mix[slot, 512:640, b * 128 : b * 128 + 128].T[:, 0:64])
            dqs[j, :, 512 + g * 128 : 640 + g * 128] = factor * jnp.concatenate(pair, axis=1)

    def run(*pairs):
        def visit(t, carry):
            s = pick([a for a, _ in pairs], t)

            @pl.when(s <= zp)
            def _():
                tile(s, pick([b for _, b in pairs], t), any(a == 0 for a, _ in pairs))

            return carry

        lax.fori_loop(0, len(pairs), visit, 0)

    def arrive(s):
        c_kzr(s).wait_recv()
        pass_on(s)

    def ready(s):
        c_kd(s).wait_recv()

    def halves(p):
        w_all(qb.at[1:3, p], r_q.at[p])
        for i in (0, 1):
            c_qh(i, p).start()

    def give(s):
        c_d(s).start()

    ready(0)
    run((0, 0))
    pl.semaphore_wait(hop.at[0], 6)
    relay(1)
    have(1, arrive)
    c_q(1, 1).start()
    c_q(2, 1).start()
    have(1, ready)
    run((1, 0))
    halves(0)
    w_all(st.at[1:3], r_st.at[0])
    c_st(3).start()
    project(1)
    run((0, 1), (1, 1))
    pl.semaphore_wait(hop.at[1], 2)
    relay(2)
    halves(1)
    project(2)
    run((0, 2))
    have(2, arrive)
    run((1, 2))
    have(2, ready)
    run((2, 0), (2, 1), (2, 2))
    pl.semaphore_wait(hop.at[2], 2)
    pl.semaphore_signal(hop.at[3], inc=1, device_id=sib, device_id_type=MESH)
    w_all(qb.at[3], r_q.at[2])
    c_st(3).wait_recv()
    project(3)
    have(3, arrive)
    run((2, 3))
    have(2, give)
    run((1, 3))
    have(1, give)
    run((0, 3))
    give(0)
    have(2, do_y1)
    have(3, ready)
    run((3, 3))
    do_dq(3)
    c_dh(0).start()
    c_dh(1).start()
    have(1, do_y1)
    run((3, 1))
    do_y1(0)
    run((3, 2))
    have(2, do_y2)

    def do_term(rel, slots):
        p = c if rel == 0 else 1 - c
        for k in (0, 1):
            got = jnp.zeros((512, 128), F32)
            wide = pl.ds(pl.multiple_of((2 * p + k) * 128, 128), 128)
            for j in slots:
                if j in (0, 3):
                    m = mix[j, 0:512, wide]
                else:
                    m = mix[1 + p, 0:512, (2 * (j - 1) + k) * 128 : (2 * (j - 1) + k + 1) * 128]
                high = m.astype(BF16)
                rest = (m - high.astype(F32)).astype(BF16)
                q = qb[j, p, :, k * 128 : k * 128 + 128]
                got = got + dot(jnp.concatenate([high, rest], axis=1), jnp.concatenate([q, q], axis=0))
            got = (factor * got).reshape(16, 4, 8, 128)
            if slots == (0,):
                got = got + term[rel, :, :, :, k * 128 : (k + 1) * 128]
            term[rel, :, :, :, k * 128 : (k + 1) * 128] = got

    do_term(1, (1, 2, 3))
    do_term(0, (1, 2, 3))
    run((3, 0))
    have(3, give)
    do_term(1, (0,))
    for j in (3, 1, 2, 0):
        c_t(j).start()
    do_term(0, (0,))
    have(1, do_y2)
    have(3, do_y1)
    for j in (3, 1, 2, 0):
        turn = (x, x1, x3, x2)[j]
        c_t(j).wait_recv()
        got = (term[0, :, turn] + termr[:, turn]).reshape(128, 256)
        if j == 0:
            wx0[...] = got
        else:
            wxs[j] = got.astype(BF16)
            c_wx(j).start()
    do_y2(0)
    have(2, do_z)
    do_dq(1)
    have(3, do_y2)
    do_dq(2)
    have(1, do_z)

    pl.semaphore_wait(hop.at[3], 1)
    got = wx0[...]
    w_all(wxr.at[1:4], r_wx.at[0])
    for j in (1, 2, 3):
        got = got + wxr[j].astype(F32)
    got = got.reshape(16, 8, 256)
    for k in (0, 1):
        rows = slice(4 * k, 4 * k + 4)
        wz[16 * k : 16 * k + 16] = jnp.concatenate([got[:, rows, 0:128], got[:, rows, 128:256]], axis=1)
    far_first = (8, 7, 9, 6, 10, 5, 11, 4, 12, 3, 13, 2, 14, 1, 15)
    for d in far_first:
        for k in (0, 1):
            c_wz(k, d).start()
    c_wz(1, 0).start()
    have(3, do_z)

    c_dh(1).wait_recv()
    dqs[1, 64:128, :] += dqh[1]
    c_dq(1).start()
    c_dh(0).wait_recv()
    dqs[2, 0:64, :] += dqh[0]
    c_dq(2).start()
    do_z(0)
    do_dq(0)

    def wait_z(d, carry):
        c_zr(d).wait_recv()
        zs[0] += zr[d]
        return carry

    lax.fori_loop(1, more + 1, wait_z, 0)
    fin[0] = zs[0].astype(BF16)
    for j in (1, 2, 3):
        c_f(j).start()

    def drain(s):
        if s < 3:

            @pl.when(more > 0)
            def _():
                c_kz(s).wait_send()

        c_kd(s).wait_send()
        c_d(s).wait_send()
        w_all(y1s.at[s], s_y1.at[s])
        w_all(y2s.at[s], s_y2.at[s])
        if s > 0:
            c_z(s).wait_send()

    for s in range(4):
        have(s, drain)
    w_all(qb.at[0:2], s_q.at[0])
    w_all(qb.at[0], s_q.at[1])
    w_all(st.at[1:3], s_st.at[0])
    c_st(3).wait_send()
    w_all(dqs.at[3], s_dh.at[0])
    w_all(termr, s_t.at[0])
    w_all(wxs.at[1:4], s_wx.at[0])

    w_all(dqr, r_dq.at[0])
    o_main[...] = dqs[0, :, 0:512] + dqr[0, :, 0:512] + dqr[1, :, 0:512]
    o_rot[...] = dqs[0, :, 512:768] + dqr[0, :, 512:768] + dqr[1, :, 512:768]

    w_all(fin.at[1:4], r_f.at[0])
    for j in range(4):
        rows = pl.ds(pl.multiple_of((y, y1, y3, y2)[j] * 32, 32), 32)
        got = zs[0] if j == 0 else fin[j].astype(F32)
        o_lat[rows, :] = got[:, 0:512]
        krots[rows, :] = got[:, 512:640]
    o_krot[...] = krots[...].T[0:64, :]
    w_all(dqs.at[1:3], s_dq.at[0])
    w_all(fin.at[1:4], s_f.at[0])
    w_all(wz.at[1:32], s_wz.at[0])

    w_all(wzr.at[1:32], r_wz.at[0])
    sums = [wz[16 * c + z] + wzr[1:16].sum(axis=0), wzr[16:32].sum(axis=0)]
    for core in (0, 1):

        @pl.when(c == core)
        def _(core=core):
            for k, at in ((0, core), (1, 1 - core)):
                o_weight[:, 256 * at : 256 * at + 128] = sums[k][0:4, :]
                o_weight[:, 256 * at + 128 : 256 * at + 256] = sums[k][4:8, :]


def put_out(*refs):
    ends, sems = refs[5:10], refs[10]
    copies = [pltpu.make_async_copy(a, b, sems.at[i]) for i, (a, b) in enumerate(zip(refs[:5], ends))]
    for copy in copies:
        copy.start()
    for copy in copies:
        copy.wait()


def per_device(query_main, query_rotary, latent, key_rotary, key_weight, value_weight, head_output, output_grad, row_logsum):
    v = pl.BlockSpec(memory_space=pltpu.VMEM)
    hbm = pl.BlockSpec(memory_space=pl.ANY)
    dma = pltpu.SemaphoreType.DMA
    scratch = [
        pltpu.VMEM((128, 128), F32),
        pltpu.VMEM((2, 512, 512), BF16),
        pltpu.VMEM((128, 512), BF16),
        pltpu.VMEM((4, 128), F32),
        pltpu.VMEM((64, 128), BF16),
        pltpu.VMEM((4, 2, 128, 640), BF16),
        pltpu.VMEM((4, 8, 512), F32),
        pltpu.VMEM((4, 8, 512), F32),
        pltpu.VMEM((4, 512, WIDE), BF16),
        pltpu.VMEM((4, 512, 512), BF16),
        pltpu.VMEM((4, 2, 128, WIDE), BF16),
        pltpu.VMEM((4, WIDE, 512), F32),
        pltpu.VMEM((4, 2, 128, WIDE), F32),
        pltpu.VMEM((4, 128, WIDE), F32),
        pltpu.VMEM((4, 2, 2, 16, WIDE), BF16),
        pltpu.VMEM((4, 2, 2, 16, WIDE), BF16),
        pltpu.VMEM((4, 2, 16, WIDE), F32),
        pltpu.VMEM((4, 2, 16, WIDE), F32),
        pltpu.VMEM((4, 32, WIDE), F32),
        pltpu.VMEM((4, 32, WIDE), F32),
        pltpu.VMEM((4, 32, WIDE), BF16),
        pltpu.VMEM((4, 128, 768), F32),
        pltpu.VMEM((2, 64, 768), F32),
        pltpu.VMEM((2, 128, 768), F32),
        pltpu.VMEM((2, 16, 4, 8, 256), F32),
        pltpu.VMEM((16, 4, 8, 256), F32),
        pltpu.VMEM((128, 256), F32),
        pltpu.VMEM((4, 128, 256), BF16),
        pltpu.VMEM((4, 128, 256), BF16),
        pltpu.VMEM((32, 8, 128), F32),
        pltpu.VMEM((32, 8, 128), F32),
        dma((6,)),
        pltpu.SemaphoreType.REGULAR((4,)),
        dma((2,)), dma((3,)),
        dma((2,)), dma((2,)),
        dma((3,)), dma((3,)),
        dma((4,)), dma((4,)),
        dma((4,)), dma((4,)),
        dma((4,)), dma((4,)),
        dma((4,)), dma((4,)),
        dma((3,)), dma((3,)),
        dma((1,)), dma((1,)),
        dma((1,)), dma((2,)),
        dma((1,)), dma((1,)),
        dma((1,)), dma((4,)),
        dma((1,)), dma((1,)),
        dma((1,)), dma((1,)),
    ]
    got = pl.pallas_call(
        body,
        out_shape=(
            pltpu.VMEM((128, 512), F32),
            pltpu.VMEM((128, 256), F32),
            pltpu.VMEM((128, 512), F32),
            pltpu.VMEM((64, 128), F32),
            pltpu.VMEM((4, 512), F32),
        ),
        in_specs=[hbm] * 9,
        out_specs=(v,) * 5,
        scratch_shapes=scratch,
        compiler_params=pltpu.CompilerParams(
            collective_id=0, has_side_effects=True, vmem_limit_bytes=56 * 1024 * 1024
        ),
    )(query_main, query_rotary, latent, key_rotary.T, key_weight, value_weight, head_output, output_grad, row_logsum)
    main, rot, lat, krot, weight = pl.pallas_call(
        put_out,
        out_shape=(
            jax.ShapeDtypeStruct((128, 512), F32),
            jax.ShapeDtypeStruct((128, 256), F32),
            jax.ShapeDtypeStruct((128, 512), F32),
            jax.ShapeDtypeStruct((64, 128), F32),
            jax.ShapeDtypeStruct((4, 512), F32),
        ),
        in_specs=[v] * 5,
        out_specs=(hbm,) * 5,
        scratch_shapes=[dma((5,))],
    )(*(pltpu.with_memory_space_constraint(a, pltpu.VMEM) for a in got))
    return main, rot, lat, krot.T, weight


def solution(mesh):
    finer = Mesh(mesh.devices.reshape(16, 4, 2, mesh.shape["tp"]), ("z", "x", "c", "y"))
    return jax.shard_map(
        per_device,
        mesh=finer,
        in_specs=(
            P(SP, "y"),
            P(SP, "y"),
            P(SP, None),
            P(SP, None),
            P(None, "y"),
            P(None, "y"),
            P(SP, "y"),
            P(SP, "y"),
            P("y", SP),
        ),
        out_specs=(P(SP, "y"), P(SP, "y"), P(SP, None), P(SP, None), P(SP, "y")),
        check_vma=False,
    )
```

```python
import jax
import jax.numpy as jnp
from jax import lax
from jax.experimental import pallas as pl
from jax.experimental.pallas import tpu as pltpu
from jax.sharding import Mesh
from jax.sharding import PartitionSpec as P

MESH = pl.DeviceIdType.MESH
SP = ("z", "x", "c")
F32 = jnp.float32
BF16 = jnp.bfloat16
WIDE = 640
LOG2E = 1.4426950408889634
NT = (((1,), (1,)), ((), ()))
TN = (((0,), (0,)), ((), ()))


def dot(a, b, dims=(((1,), (0,)), ((), ()))):
    return lax.dot_general(a, b, dims, preferred_element_type=F32)


def pick(table, t):
    out = jnp.int32(0)
    for k, v in enumerate(table):
        if v:
            out = out + jnp.where(t == k, v, 0)
    return out


def body(
    qm, qr, lat, krt, kwh, vwh, hoh, og, lsh,
    o_main, o_rot, o_lat, o_krot, o_weight,
    krots, kv, ho, ls, krv, qb, st, sts, qc, qt, gr, keys, mix, part, turned, dsum, y1s, y1r, y2s, y2r, zs, zr, fin,
    dqs, dqh, dqr, term, termr, wx0, wxs, wxr, wz, wzr,
    s_loc, hop, s_q, r_q, s_st, r_st, s_kz, r_kz, s_kd, r_kd, s_d, r_d, s_y1, r_y1, s_y2, r_y2,
    s_z, r_z, s_f, r_f, s_dh, r_dh, s_dq, r_dq, s_t, r_t, s_wx, r_wx, s_wz, r_wz,
):
    z, x, c, y = (lax.axis_index(a) for a in ("z", "x", "c", "y"))
    factor = 192.0 ** (-0.5)
    zp = jnp.where(z < 3, z, (z + 1) % 4)
    planes = jnp.where(z < 3, 3, jnp.where(z < 15, 4, 1))
    more = planes - 1 - zp
    sib = {"c": 1 - c}
    x1, x3, x2 = x + 1 - 2 * (x % 2), 3 - x, (x + 2) % 4
    y1, y3, y2 = y + 1 - 2 * (y % 2), 3 - y, (y + 2) % 4
    xdev = (None, {"x": x1}, {"x": x3}, {"x": x2})
    ydev = (None, {"y": y1}, {"y": y3}, {"y": y2})

    def remote(src, dst, ss, rs, dev):
        return pltpu.make_async_remote_copy(
            src_ref=src, dst_ref=dst, send_sem=ss, recv_sem=rs, device_id=dev, device_id_type=MESH
        )

    def c_q(j, p):
        return remote(qb.at[0, p], qb.at[j, p], s_q.at[0], r_q.at[p], xdev[j])

    def c_qh(i, p):
        rows = pl.ds(64 * i, 64)
        return remote(qb.at[1 + i, p, rows], qb.at[3, p, rows], s_q.at[1], r_q.at[2], xdev[2 - i])

    def c_st(j):
        if j == 3:
            return remote(st.at[1], st.at[3], s_st.at[1], r_st.at[1], xdev[2])
        return remote(st.at[0], st.at[j], s_st.at[0], r_st.at[0], xdev[j])

    def c_kz(s):
        return remote(keys.at[s, 0], keys.at[s + 1, 0], s_kz.at[s], r_kz.at[s], {"z": z + 1})

    def c_kzr(s):
        return remote(keys.at[s - 1, 0], keys.at[s, 0], s_kz.at[s - 1], r_kz.at[s - 1], {"z": z - 1})

    def c_kd(s):
        return remote(keys.at[s, 0], keys.at[s, 1], s_kd.at[s], r_kd.at[s], sib)

    def c_d(s):
        return remote(part.at[s, 1], dsum.at[s], s_d.at[s], r_d.at[s], sib)

    def c_y1(s, g):
        return remote(y1s.at[s, g], y1r.at[s, g], s_y1.at[s], r_y1.at[s], ydev[1 + g])

    def c_y2(s, g):
        return remote(y2s.at[s, g], y2r.at[s, g], s_y2.at[s], r_y2.at[s], ydev[2 - g])

    def c_z(s):
        return remote(zs.at[s], zr.at[s], s_z.at[s - 1], r_z.at[s - 1], {"z": z - s})

    def c_zr(s):
        return remote(zs.at[s], zr.at[s], s_z.at[s - 1], r_z.at[s - 1], {"z": z + s})

    def c_f(j):
        return remote(fin.at[0], fin.at[j], s_f.at[0], r_f.at[0], ydev[j])

    def c_dh(i):
        rows = pl.ds(64 * i, 64)
        return remote(dqs.at[3, rows], dqh.at[i], s_dh.at[0], r_dh.at[i], xdev[1 + i])

    def c_dq(j):
        return remote(dqs.at[j], dqr.at[j - 1], s_dq.at[0], r_dq.at[0], xdev[j])

    def c_t(j):
        turn = (x, x1, x3, x2)[j]
        return remote(term.at[1 - c, :, turn], termr.at[:, turn], s_t.at[0], r_t.at[j], sib)

    def c_wx(j):
        return remote(wxs.at[j], wxr.at[j], s_wx.at[0], r_wx.at[0], xdev[j])

    def c_wz(k, d):
        to = (z + d) % 16
        own = c if k == 0 else 1 - c
        dev = {"z": to, "c": own}
        return remote(wz.at[own * 16 + to], wzr.at[16 * k + d], s_wz.at[0], r_wz.at[0], dev)

    def w_all(ref, sem):
        pltpu.make_async_copy(ref, ref, sem).wait()

    barrier = pltpu.get_barrier_semaphore()
    for dev in (sib, *xdev[1:3], *ydev[1:3], {"z": (z + 1) % 16}, {"z": (z + 15) % 16}):
        pl.semaphore_signal(barrier, inc=1, device_id=dev, device_id_type=MESH)
    first = [
        (krt, krv, 0),
        (lat, keys.at[0, 0, :, 0:512], 1),
        (qm.at[:, 0:256], qb.at[0, 0, :, 0:256], 2),
        (qr.at[:, 0:128], qb.at[0, 0, :, 256:384], 2),
        (og.at[:, 0:256], qb.at[0, 0, :, 384:640], 2),
        (qm.at[:, 256:512], qb.at[0, 1, :, 0:256], 2),
        (qr.at[:, 128:256], qb.at[0, 1, :, 256:384], 2),
        (og.at[:, 256:512], qb.at[0, 1, :, 384:640], 2),
        (kwh, kv.at[0], 3),
        (vwh, kv.at[1], 3),
        (hoh, ho, 4),
        (lsh, ls, 5),
    ]
    kw, vw = kv.at[0], kv.at[1]
    loads = [pltpu.make_async_copy(a, b, s_loc.at[i]) for a, b, i in first]
    for copy in loads:
        copy.start()
    loads[0].wait()
    keys[0, 0, :, 512:WIDE] = jnp.concatenate([krv[...].T, jnp.zeros((128, 64), BF16)], axis=1)
    loads[1].wait()
    w_all(qb.at[0], s_loc.at[2])
    pl.semaphore_wait(barrier, 7)

    def relay(i):
        for d in (1 << i, 16 - (1 << i)):
            pl.semaphore_signal(hop.at[i], inc=1, device_id={"z": (z + d) % 16}, device_id_type=MESH)
        if i == 0:
            for dev in (*xdev[1:3], *ydev[1:3]):
                pl.semaphore_signal(hop.at[i], inc=1, device_id=dev, device_id_type=MESH)

    def pass_on(s):
        if s < 3:

            @pl.when(more > 0)
            def _():
                c_kz(s).start()

        c_kd(s).start()

    c_q(1, 0).start()
    c_q(2, 0).start()
    pass_on(0)
    relay(0)

    def rows_of(slot):
        if slot in (0, 3):
            return [(slot, h) for h in range(4)]
        return [(j, 2 * (slot - 1) + h) for j in (1, 2) for h in (0, 1)]

    def place_of(j, h):
        if j in (0, 3):
            return j, h
        return 1 + h // 2, 2 * (j - 1) + h % 2

    w_all(kv, s_loc.at[3])
    for copy in loads[10:]:
        copy.wait()
    ones = jnp.ones((8, 128), F32)
    for h in range(4):
        cols = pl.ds(h * 128, 128)
        prod = ho[:, cols].astype(F32) * qb[0, h // 2, :, 384 + h % 2 * 128 : 512 + h % 2 * 128].astype(F32)
        sums = lax.dot_general(
            ones, prod, NT, precision=lax.Precision.HIGHEST, preferred_element_type=F32
        )
        st[0, 1:2, cols] = sums[0:1, :]
        st[0, 0:1, cols] = LOG2E * ls[h : h + 1, :]
    for j in (1, 2):
        c_st(j).start()

    def project(slot):
        for b, (j, h) in enumerate(rows_of(slot)):
            p, k = h // 2, h % 2
            cols = pl.ds(h * 128, 128)
            rows = pl.ds(b * 128, 128)
            qc[slot, rows, 0:512] = dot(qb[j, p, :, k * 128 : k * 128 + 128], kw[:, cols], NT).astype(BF16)
            gr[slot, rows, :] = dot(qb[j, p, :, 384 + k * 128 : 512 + k * 128], vw[:, cols], NT).astype(BF16)
            rot = qb[j, p, :, 256 + k * 64 : 320 + k * 64]
            qt[slot, :, rows] = rot.T
            qc[slot, rows, 512:WIDE] = jnp.concatenate([rot, jnp.zeros((128, 64), BF16)], axis=1)
            sts[slot, 0:2, rows] = st[j, 0:2, cols]

    project(0)
    mix[...] = jnp.zeros_like(mix)
    part[...] = jnp.zeros_like(part)
    turned[...] = jnp.zeros_like(turned)

    def tile(s, j, masked):
        kt = keys[s].reshape(256, WIDE)
        turn_a = jnp.where(j == 0, x, jnp.where(j == 3, x2, x1))
        turn_b = jnp.where(j == 0, x, jnp.where(j == 3, x2, x3))
        far = jnp.where(s > 0, 1 << 20, 0)
        first = (2 * x + c) * 128 - far
        second = (2 * x + 1 - c) * 128 - 128 - far
        k_row = lax.broadcasted_iota(jnp.int32, (256, 1), 0)
        k_place = jnp.where(k_row < 128, k_row + first, k_row + second)
        q_col = lax.broadcasted_iota(jnp.int32, (1, 512), 1)
        q_place = q_col % 128 + jnp.where(q_col < 256, 2 * turn_a + c, 2 * turn_b + c) * 128
        scores = dot(kt, qc[j], NT)
        weights = jnp.exp2((factor * LOG2E) * scores - sts[j, 0:1, :])
        if masked:
            weights = jnp.where(k_place <= q_place, weights, 0.0)
        slopes = dot(kt[:, 0:512], gr[j], NT)
        dscores = weights * (slopes - sts[j, 1:2, :])
        w_low = weights.astype(BF16)
        d_low = dscores.astype(BF16)
        mix[j, 0:576, :] += dot(kt[:, 0:576], d_low, TN)
        main = factor * dot(d_low, qc[j, :, 0:512]) + dot(w_low, gr[j])
        part[s, :, :, 0:512] += main.reshape(2, 128, 512)
        turned[s] += factor * dot(qt[j], d_low, NT)

    def own(s, g, yy):
        rows = pl.ds(pl.multiple_of(yy * 32 + 16 * g, 16), 16)
        return part[s, 0, rows, :] + dsum[s, rows, :]

    def do_y1(s):
        c_d(s).wait_recv()
        for g in (0, 1):
            y1s[s, g, 0] = own(s, g, (y1, y3)[g]).astype(BF16)
            y1s[s, g, 1] = own(s, g, y2).astype(BF16)
            c_y1(s, g).start()

    def do_y2(s):
        w_all(y1r.at[s], r_y1.at[s])
        for g in (0, 1):
            y2s[s, g] = own(s, g, (y3, y1)[g]) + y1r[s, g, 1].astype(F32)
            c_y2(s, g).start()

    def do_z(s):
        w_all(y2r.at[s], r_y2.at[s])
        for g in (0, 1):
            zs[s, 16 * g : 16 * g + 16, :] = own(s, g, y) + y1r[s, g, 0].astype(F32) + y2r[s, g]
        if s > 0:
            c_z(s).start()

    def have(s, act):
        @pl.when(zp >= s)
        def _():
            act(s)

    def do_dq(j):
        for h in range(4):
            cols = pl.ds(h * 128, 128)
            slot, b = place_of(j, h)
            m = mix[slot, 0:512, b * 128 : b * 128 + 128]
            high = m.astype(BF16)
            rest = (m - high.astype(F32)).astype(BF16)
            got = dot(high, kw[:, cols], TN) + dot(rest, kw[:, cols], TN)
            dqs[j, :, cols] = factor * got
        for g in range(2):
            pair = []
            for h in (2 * g, 2 * g + 1):
                slot, b = place_of(j, h)
                pair.append(mix[slot, 512:640, b * 128 : b * 128 + 128].T[:, 0:64])
            dqs[j, :, 512 + g * 128 : 640 + g * 128] = factor * jnp.concatenate(pair, axis=1)

    def run(*pairs):
        def visit(t, carry):
            s = pick([a for a, _ in pairs], t)

            @pl.when(s <= zp)
            def _():
                tile(s, pick([b for _, b in pairs], t), any(a == 0 for a, _ in pairs))

            return carry

        lax.fori_loop(0, len(pairs), visit, 0)

    def arrive(s):
        c_kzr(s).wait_recv()
        pass_on(s)

    def ready(s):
        c_kd(s).wait_recv()

    def halves(p):
        w_all(qb.at[1:3, p], r_q.at[p])
        for i in (0, 1):
            c_qh(i, p).start()

    def give(s):
        for k in (1, 0):
            rot = turned[s, :, 128 * k : 128 * k + 128].T
            part[s, k, :, 512:WIDE] = jnp.concatenate([rot, jnp.zeros((128, 64), F32)], axis=1)
            if k == 1:
                c_d(s).start()

    ready(0)
    run((0, 0))
    c_q(1, 1).start()
    c_q(2, 1).start()
    pl.semaphore_wait(hop.at[0], 6)
    relay(1)
    have(1, arrive)
    have(1, ready)
    run((1, 0))
    halves(0)
    w_all(st.at[1:3], r_st.at[0])
    c_st(3).start()
    project(1)
    run((0, 1), (1, 1))
    pl.semaphore_wait(hop.at[1], 2)
    relay(2)
    halves(1)
    project(2)
    run((0, 2))
    have(2, arrive)
    run((1, 2))
    have(2, ready)
    run((2, 0), (2, 1))
    pl.semaphore_wait(hop.at[2], 2)
    pl.semaphore_signal(hop.at[3], inc=1, device_id=sib, device_id_type=MESH)
    w_all(qb.at[3], r_q.at[2])
    c_st(3).wait_recv()
    project(3)
    run((2, 3))
    have(3, arrive)
    run((1, 3))
    have(1, give)
    run((0, 3))
    give(0)
    have(3, ready)
    run((3, 3))
    do_dq(3)
    c_dh(0).start()
    c_dh(1).start()
    have(1, do_y1)
    run((3, 1))
    do_y1(0)

    def do_term(p, slots, fresh):
        for k in (0, 1):
            got = jnp.zeros((512, 128), F32)
            for j in slots:
                slot, b = place_of(j, 2 * p + k)
                m = mix[slot, 0:512, b * 128 : b * 128 + 128]
                high = m.astype(BF16)
                rest = (m - high.astype(F32)).astype(BF16)
                q = qb[j, p, :, k * 128 : k * 128 + 128]
                got = got + dot(jnp.concatenate([high, rest], axis=1), jnp.concatenate([q, q], axis=0))
            got = (factor * got).reshape(16, 4, 8, 128)
            if not fresh:
                got = got + term[p, :, :, :, k * 128 : (k + 1) * 128]
            term[p, :, :, :, k * 128 : (k + 1) * 128] = got

    def hand_over(core):
        @pl.when(c == core)
        def _():
            for j in (3, 1, 2, 0):
                c_t(j).start()

    do_term(0, (1, 2, 3), True)
    run((3, 0))
    do_term(0, (0,), False)
    hand_over(1)
    do_term(1, (0, 3), True)
    run((3, 2))
    have(3, give)
    run((2, 2))
    do_term(1, (1, 2), False)
    hand_over(0)
    have(3, do_y1)
    have(2, give)
    have(1, do_y2)
    for j in (3, 1, 2, 0):
        turn = (x, x1, x3, x2)[j]
        c_t(j).wait_recv()
        got = (term[c, :, turn] + termr[:, turn]).reshape(128, 256)
        if j == 0:
            wx0[...] = got
        else:
            wxs[j] = got.astype(BF16)
            c_wx(j).start()
    have(2, do_y1)
    do_y2(0)
    do_dq(1)
    do_dq(2)
    have(3, do_y2)
    have(1, do_z)

    pl.semaphore_wait(hop.at[3], 1)
    got = wx0[...]
    w_all(wxr.at[1:4], r_wx.at[0])
    for j in (1, 2, 3):
        got = got + wxr[j].astype(F32)
    got = got.reshape(16, 8, 256)
    for k in (0, 1):
        rows = slice(4 * k, 4 * k + 4)
        wz[16 * k : 16 * k + 16] = jnp.concatenate([got[:, rows, 0:128], got[:, rows, 128:256]], axis=1)
    far_first = (8, 7, 9, 6, 10, 5, 11, 4, 12, 3, 13, 2, 14, 1, 15)
    for d in far_first:
        for k in (0, 1):
            c_wz(k, d).start()
    c_wz(1, 0).start()
    have(3, do_z)
    have(2, do_y2)

    c_dh(1).wait_recv()
    dqs[1, 64:128, :] += dqh[1]
    c_dq(1).start()
    c_dh(0).wait_recv()
    dqs[2, 0:64, :] += dqh[0]
    c_dq(2).start()
    do_z(0)
    do_dq(0)
    have(2, do_z)

    def wait_z(d, carry):
        c_zr(d).wait_recv()
        zs[0] += zr[d]
        return carry

    lax.fori_loop(1, more + 1, wait_z, 0)
    fin[0] = zs[0].astype(BF16)
    for j in (1, 2, 3):
        c_f(j).start()

    def drain(s):
        if s < 3:

            @pl.when(more > 0)
            def _():
                c_kz(s).wait_send()

        c_kd(s).wait_send()
        c_d(s).wait_send()
        w_all(y1s.at[s], s_y1.at[s])
        w_all(y2s.at[s], s_y2.at[s])
        if s > 0:
            c_z(s).wait_send()

    for s in range(4):
        have(s, drain)
    w_all(qb.at[0:2], s_q.at[0])
    w_all(qb.at[0], s_q.at[1])
    w_all(st.at[1:3], s_st.at[0])
    c_st(3).wait_send()
    w_all(dqs.at[3], s_dh.at[0])
    w_all(termr, s_t.at[0])
    w_all(wxs.at[1:4], s_wx.at[0])

    w_all(dqr, r_dq.at[0])
    o_main[...] = dqs[0, :, 0:512] + dqr[0, :, 0:512] + dqr[1, :, 0:512]
    o_rot[...] = dqs[0, :, 512:768] + dqr[0, :, 512:768] + dqr[1, :, 512:768]

    w_all(fin.at[1:4], r_f.at[0])
    for j in range(4):
        rows = pl.ds(pl.multiple_of((y, y1, y3, y2)[j] * 32, 32), 32)
        got = zs[0] if j == 0 else fin[j].astype(F32)
        o_lat[rows, :] = got[:, 0:512]
        krots[rows, :] = got[:, 512:640]
    o_krot[...] = krots[...].T[0:64, :]
    w_all(dqs.at[1:3], s_dq.at[0])
    w_all(fin.at[1:4], s_f.at[0])
    w_all(wz.at[1:32], s_wz.at[0])

    w_all(wzr.at[1:32], r_wz.at[0])
    sums = [wz[16 * c + z] + wzr[1:16].sum(axis=0), wzr[16:32].sum(axis=0)]
    for core in (0, 1):

        @pl.when(c == core)
        def _(core=core):
            for k, at in ((0, core), (1, 1 - core)):
                o_weight[:, 256 * at : 256 * at + 128] = sums[k][0:4, :]
                o_weight[:, 256 * at + 128 : 256 * at + 256] = sums[k][4:8, :]


def put_out(*refs):
    ends, sems = refs[5:10], refs[10]
    copies = [pltpu.make_async_copy(a, b, sems.at[i]) for i, (a, b) in enumerate(zip(refs[:5], ends))]
    for copy in copies:
        copy.start()
    for copy in copies:
        copy.wait()


def per_device(query_main, query_rotary, latent, key_rotary, key_weight, value_weight, head_output, output_grad, row_logsum):
    v = pl.BlockSpec(memory_space=pltpu.VMEM)
    hbm = pl.BlockSpec(memory_space=pl.ANY)
    dma = pltpu.SemaphoreType.DMA
    scratch = [
        pltpu.VMEM((128, 128), F32),
        pltpu.VMEM((2, 512, 512), BF16),
        pltpu.VMEM((128, 512), BF16),
        pltpu.VMEM((4, 128), F32),
        pltpu.VMEM((64, 128), BF16),
        pltpu.VMEM((4, 2, 128, 640), BF16),
        pltpu.VMEM((4, 8, 512), F32),
        pltpu.VMEM((4, 8, 512), F32),
        pltpu.VMEM((4, 512, WIDE), BF16),
        pltpu.VMEM((4, 64, 512), BF16),
        pltpu.VMEM((4, 512, 512), BF16),
        pltpu.VMEM((4, 2, 128, WIDE), BF16),
        pltpu.VMEM((4, WIDE, 512), F32),
        pltpu.VMEM((4, 2, 128, WIDE), F32),
        pltpu.VMEM((4, 64, 256), F32),
        pltpu.VMEM((4, 128, WIDE), F32),
        pltpu.VMEM((4, 2, 2, 16, WIDE), BF16),
        pltpu.VMEM((4, 2, 2, 16, WIDE), BF16),
        pltpu.VMEM((4, 2, 16, WIDE), F32),
        pltpu.VMEM((4, 2, 16, WIDE), F32),
        pltpu.VMEM((4, 32, WIDE), F32),
        pltpu.VMEM((4, 32, WIDE), F32),
        pltpu.VMEM((4, 32, WIDE), BF16),
        pltpu.VMEM((4, 128, 768), F32),
        pltpu.VMEM((2, 64, 768), F32),
        pltpu.VMEM((2, 128, 768), F32),
        pltpu.VMEM((2, 16, 4, 8, 256), F32),
        pltpu.VMEM((16, 4, 8, 256), F32),
        pltpu.VMEM((128, 256), F32),
        pltpu.VMEM((4, 128, 256), BF16),
        pltpu.VMEM((4, 128, 256), BF16),
        pltpu.VMEM((32, 8, 128), F32),
        pltpu.VMEM((32, 8, 128), F32),
        dma((6,)),
        pltpu.SemaphoreType.REGULAR((4,)),
        dma((2,)), dma((3,)),
        dma((2,)), dma((2,)),
        dma((3,)), dma((3,)),
        dma((4,)), dma((4,)),
        dma((4,)), dma((4,)),
        dma((4,)), dma((4,)),
        dma((4,)), dma((4,)),
        dma((3,)), dma((3,)),
        dma((1,)), dma((1,)),
        dma((1,)), dma((2,)),
        dma((1,)), dma((1,)),
        dma((1,)), dma((4,)),
        dma((1,)), dma((1,)),
        dma((1,)), dma((1,)),
    ]
    got = pl.pallas_call(
        body,
        out_shape=(
            pltpu.VMEM((128, 512), F32),
            pltpu.VMEM((128, 256), F32),
            pltpu.VMEM((128, 512), F32),
            pltpu.VMEM((64, 128), F32),
            pltpu.VMEM((4, 512), F32),
        ),
        in_specs=[hbm] * 9,
        out_specs=(v,) * 5,
        scratch_shapes=scratch,
        compiler_params=pltpu.CompilerParams(
            collective_id=0, has_side_effects=True, vmem_limit_bytes=56 * 1024 * 1024
        ),
    )(query_main, query_rotary, latent, key_rotary.T, key_weight, value_weight, head_output, output_grad, row_logsum)
    main, rot, lat, krot, weight = pl.pallas_call(
        put_out,
        out_shape=(
            jax.ShapeDtypeStruct((128, 512), F32),
            jax.ShapeDtypeStruct((128, 256), F32),
            jax.ShapeDtypeStruct((128, 512), F32),
            jax.ShapeDtypeStruct((64, 128), F32),
            jax.ShapeDtypeStruct((4, 512), F32),
        ),
        in_specs=[v] * 5,
        out_specs=(hbm,) * 5,
        scratch_shapes=[dma((5,))],
    )(*(pltpu.with_memory_space_constraint(a, pltpu.VMEM) for a in got))
    return main, rot, lat, krot.T, weight


def solution(mesh):
    finer = Mesh(mesh.devices.reshape(16, 4, 2, mesh.shape["tp"]), ("z", "x", "c", "y"))
    return jax.shard_map(
        per_device,
        mesh=finer,
        in_specs=(
            P(SP, "y"),
            P(SP, "y"),
            P(SP, None),
            P(SP, None),
            P(None, "y"),
            P(None, "y"),
            P(SP, "y"),
            P(SP, "y"),
            P("y", SP),
        ),
        out_specs=(P(SP, "y"), P(SP, "y"), P(SP, None), P(SP, None), P(SP, "y")),
        check_vma=False,
    )
```

```python
import jax
import jax.numpy as jnp
from jax import lax
from jax.experimental import pallas as pl
from jax.experimental.pallas import tpu as pltpu
from jax.sharding import Mesh
from jax.sharding import PartitionSpec as P

MESH = pl.DeviceIdType.MESH
SP = ("z", "x", "c")
F32 = jnp.float32
BF16 = jnp.bfloat16
WIDE = 640
LOG2E = 1.4426950408889634
NT = (((1,), (1,)), ((), ()))
TN = (((0,), (0,)), ((), ()))


def dot(a, b, dims=(((1,), (0,)), ((), ()))):
    return lax.dot_general(a, b, dims, preferred_element_type=F32)


def pick(table, t):
    out = jnp.int32(0)
    for k, v in enumerate(table):
        if v:
            out = out + jnp.where(t == k, v, 0)
    return out


def body(
    qm, qr, lat, krt, kwh, vwh, hoh, og, lsh,
    o_main, o_rot, o_lat, o_krot, o_weight,
    krots, kv, ho, ls, krv, qb, st, sts, qc, qt, gr, keys, mix, part, turned, dsum, y1s, y1r, y2s, y2r, zs, zr, fin,
    dqs, dqh, dqr, term, termr, wx0, wxs, wxr, wz, wzr,
    s_loc, hop, s_q, r_q, s_st, r_st, s_kz, r_kz, s_kd, r_kd, s_d, r_d, s_y1, r_y1, s_y2, r_y2,
    s_z, r_z, s_f, r_f, s_dh, r_dh, s_dq, r_dq, s_t, r_t, s_wx, r_wx, s_wz, r_wz,
):
    z, x, c, y = (lax.axis_index(a) for a in ("z", "x", "c", "y"))
    factor = 192.0 ** (-0.5)
    zp = jnp.where(z < 3, z, (z + 1) % 4)
    planes = jnp.where(z < 3, 3, jnp.where(z < 15, 4, 1))
    more = planes - 1 - zp
    sib = {"c": 1 - c}
    x1, x3, x2 = x + 1 - 2 * (x % 2), 3 - x, (x + 2) % 4
    y1, y3, y2 = y + 1 - 2 * (y % 2), 3 - y, (y + 2) % 4
    xdev = (None, {"x": x1}, {"x": x3}, {"x": x2})
    ydev = (None, {"y": y1}, {"y": y3}, {"y": y2})

    def remote(src, dst, ss, rs, dev):
        return pltpu.make_async_remote_copy(
            src_ref=src, dst_ref=dst, send_sem=ss, recv_sem=rs, device_id=dev, device_id_type=MESH
        )

    def c_q(j, p):
        return remote(qb.at[0, p], qb.at[j, p], s_q.at[0], r_q.at[p], xdev[j])

    def c_qh(i, p):
        rows = pl.ds(64 * i, 64)
        return remote(qb.at[1 + i, p, rows], qb.at[3, p, rows], s_q.at[1], r_q.at[2], xdev[2 - i])

    def c_st(j):
        if j == 3:
            return remote(st.at[1], st.at[3], s_st.at[1], r_st.at[1], xdev[2])
        return remote(st.at[0], st.at[j], s_st.at[0], r_st.at[0], xdev[j])

    def c_kz(s):
        return remote(keys.at[s, 0], keys.at[s + 1, 0], s_kz.at[s], r_kz.at[s], {"z": z + 1})

    def c_kzr(s):
        return remote(keys.at[s - 1, 0], keys.at[s, 0], s_kz.at[s - 1], r_kz.at[s - 1], {"z": z - 1})

    def c_kd(s):
        return remote(keys.at[s, 0], keys.at[s, 1], s_kd.at[s], r_kd.at[s], sib)

    def c_d(s):
        return remote(part.at[s, 1], dsum.at[s], s_d.at[s], r_d.at[s], sib)

    def c_y1(s, g):
        return remote(y1s.at[s, g], y1r.at[s, g], s_y1.at[s], r_y1.at[s], ydev[1 + g])

    def c_y2(s, g):
        return remote(y2s.at[s, g], y2r.at[s, g], s_y2.at[s], r_y2.at[s], ydev[2 - g])

    def c_z(s):
        return remote(zs.at[s], zr.at[s], s_z.at[s - 1], r_z.at[s - 1], {"z": z - s})

    def c_zr(s):
        return remote(zs.at[s], zr.at[s], s_z.at[s - 1], r_z.at[s - 1], {"z": z + s})

    def c_f(j):
        return remote(fin.at[0], fin.at[j], s_f.at[0], r_f.at[0], ydev[j])

    def c_dh(i):
        rows = pl.ds(64 * i, 64)
        return remote(dqs.at[3, rows], dqh.at[i], s_dh.at[0], r_dh.at[i], xdev[1 + i])

    def c_dq(j):
        return remote(dqs.at[j], dqr.at[j - 1], s_dq.at[0], r_dq.at[0], xdev[j])

    def c_t(j):
        turn = (x, x1, x3, x2)[j]
        return remote(term.at[1 - c, :, turn], termr.at[:, turn], s_t.at[0], r_t.at[j], sib)

    def c_wx(j):
        return remote(wxs.at[j], wxr.at[j], s_wx.at[0], r_wx.at[0], xdev[j])

    def c_wz(k, d):
        to = (z + d) % 16
        own = c if k == 0 else 1 - c
        dev = {"z": to, "c": own}
        return remote(wz.at[own * 16 + to], wzr.at[16 * k + d], s_wz.at[0], r_wz.at[0], dev)

    def w_all(ref, sem):
        pltpu.make_async_copy(ref, ref, sem).wait()

    barrier = pltpu.get_barrier_semaphore()
    for dev in (sib, *xdev[1:3], *ydev[1:3], {"z": (z + 1) % 16}, {"z": (z + 15) % 16}):
        pl.semaphore_signal(barrier, inc=1, device_id=dev, device_id_type=MESH)
    first = [
        (krt, krv, 0),
        (lat, keys.at[0, 0, :, 0:512], 1),
        (qm.at[:, 0:256], qb.at[0, 0, :, 0:256], 2),
        (qr.at[:, 0:128], qb.at[0, 0, :, 256:384], 2),
        (og.at[:, 0:256], qb.at[0, 0, :, 384:640], 2),
        (qm.at[:, 256:512], qb.at[0, 1, :, 0:256], 2),
        (qr.at[:, 128:256], qb.at[0, 1, :, 256:384], 2),
        (og.at[:, 256:512], qb.at[0, 1, :, 384:640], 2),
        (kwh, kv.at[0], 3),
        (vwh, kv.at[1], 3),
        (hoh, ho, 4),
        (lsh, ls, 5),
    ]
    kw, vw = kv.at[0], kv.at[1]
    loads = [pltpu.make_async_copy(a, b, s_loc.at[i]) for a, b, i in first]
    for copy in loads:
        copy.start()
    loads[0].wait()
    keys[0, 0, :, 512:WIDE] = jnp.concatenate([krv[...].T, jnp.zeros((128, 64), BF16)], axis=1)
    loads[1].wait()
    w_all(qb.at[0], s_loc.at[2])
    pl.semaphore_wait(barrier, 7)

    def relay(i):
        for d in (1 << i, 16 - (1 << i)):
            pl.semaphore_signal(hop.at[i], inc=1, device_id={"z": (z + d) % 16}, device_id_type=MESH)
        if i == 0:
            for dev in (*xdev[1:3], *ydev[1:3]):
                pl.semaphore_signal(hop.at[i], inc=1, device_id=dev, device_id_type=MESH)

    def pass_on(s):
        if s < 3:

            @pl.when(more > 0)
            def _():
                c_kz(s).start()

        c_kd(s).start()

    c_q(1, 0).start()
    c_q(2, 0).start()
    pass_on(0)
    relay(0)

    def rows_of(slot):
        if slot in (0, 3):
            return [(slot, h) for h in range(4)]
        return [(j, 2 * (slot - 1) + h) for j in (1, 2) for h in (0, 1)]

    def place_of(j, h):
        if j in (0, 3):
            return j, h
        return 1 + h // 2, 2 * (j - 1) + h % 2

    w_all(kv, s_loc.at[3])
    for copy in loads[10:]:
        copy.wait()
    ones = jnp.ones((8, 128), F32)
    for h in range(4):
        cols = pl.ds(h * 128, 128)
        prod = ho[:, cols].astype(F32) * qb[0, h // 2, :, 384 + h % 2 * 128 : 512 + h % 2 * 128].astype(F32)
        sums = lax.dot_general(
            ones, prod, NT, precision=lax.Precision.HIGHEST, preferred_element_type=F32
        )
        st[0, 1:2, cols] = sums[0:1, :]
        st[0, 0:1, cols] = LOG2E * ls[h : h + 1, :]
    for j in (1, 2):
        c_st(j).start()

    def project(slot):
        for b, (j, h) in enumerate(rows_of(slot)):
            p, k = h // 2, h % 2
            cols = pl.ds(h * 128, 128)
            rows = pl.ds(b * 128, 128)
            qc[slot, rows, 0:512] = dot(qb[j, p, :, k * 128 : k * 128 + 128], kw[:, cols], NT).astype(BF16)
            gr[slot, rows, :] = dot(qb[j, p, :, 384 + k * 128 : 512 + k * 128], vw[:, cols], NT).astype(BF16)
            rot = qb[j, p, :, 256 + k * 64 : 320 + k * 64]
            qt[slot, :, rows] = rot.T
            qc[slot, rows, 512:WIDE] = jnp.concatenate([rot, jnp.zeros((128, 64), BF16)], axis=1)
            sts[slot, 0:2, rows] = st[j, 0:2, cols]

    project(0)
    mix[...] = jnp.zeros_like(mix)
    part[...] = jnp.zeros_like(part)
    turned[...] = jnp.zeros_like(turned)

    def tile(s, j, masked):
        kt = keys[s].reshape(256, WIDE)
        turn_a = jnp.where(j == 0, x, jnp.where(j == 3, x2, x1))
        turn_b = jnp.where(j == 0, x, jnp.where(j == 3, x2, x3))
        far = jnp.where(s > 0, 1 << 20, 0)
        first = (2 * x + c) * 128 - far
        second = (2 * x + 1 - c) * 128 - 128 - far
        k_row = lax.broadcasted_iota(jnp.int32, (256, 1), 0)
        k_place = jnp.where(k_row < 128, k_row + first, k_row + second)
        q_col = lax.broadcasted_iota(jnp.int32, (1, 512), 1)
        q_place = q_col % 128 + jnp.where(q_col < 256, 2 * turn_a + c, 2 * turn_b + c) * 128
        scores = dot(kt, qc[j], NT)
        weights = jnp.exp2((factor * LOG2E) * scores - sts[j, 0:1, :])
        if masked:
            weights = jnp.where(k_place <= q_place, weights, 0.0)
        slopes = dot(kt[:, 0:512], gr[j], NT)
        dscores = weights * (slopes - sts[j, 1:2, :])
        w_low = weights.astype(BF16)
        d_low = dscores.astype(BF16)
        mix[j, 0:576, :] += dot(kt[:, 0:576], d_low, TN)
        main = factor * dot(d_low, qc[j, :, 0:512]) + dot(w_low, gr[j])
        part[s, :, :, 0:512] += main.reshape(2, 128, 512)
        turned[s] += factor * dot(qt[j], d_low, NT)

    def own(s, g, yy):
        rows = pl.ds(pl.multiple_of(yy * 32 + 16 * g, 16), 16)
        return part[s, 0, rows, :] + dsum[s, rows, :]

    def do_y1(s):
        c_d(s).wait_recv()
        for g in (0, 1):
            y1s[s, g, 0] = own(s, g, (y1, y3)[g]).astype(BF16)
            y1s[s, g, 1] = own(s, g, y2).astype(BF16)
            c_y1(s, g).start()

    def do_y2(s):
        w_all(y1r.at[s], r_y1.at[s])
        for g in (0, 1):
            y2s[s, g] = own(s, g, (y3, y1)[g]) + y1r[s, g, 1].astype(F32)
            c_y2(s, g).start()

    def do_z(s):
        w_all(y2r.at[s], r_y2.at[s])
        for g in (0, 1):
            zs[s, 16 * g : 16 * g + 16, :] = own(s, g, y) + y1r[s, g, 0].astype(F32) + y2r[s, g]
        if s > 0:
            c_z(s).start()

    def have(s, act):
        @pl.when(zp >= s)
        def _():
            act(s)

    def do_dq(j):
        for h in range(4):
            cols = pl.ds(h * 128, 128)
            slot, b = place_of(j, h)
            m = mix[slot, 0:512, b * 128 : b * 128 + 128]
            high = m.astype(BF16)
            rest = (m - high.astype(F32)).astype(BF16)
            got = dot(high, kw[:, cols], TN) + dot(rest, kw[:, cols], TN)
            dqs[j, :, cols] = factor * got
        for g in range(2):
            pair = []
            for h in (2 * g, 2 * g + 1):
                slot, b = place_of(j, h)
                pair.append(mix[slot, 512:640, b * 128 : b * 128 + 128].T[:, 0:64])
            dqs[j, :, 512 + g * 128 : 640 + g * 128] = factor * jnp.concatenate(pair, axis=1)

    def run(*pairs):
        def visit(t, carry):
            s = pick([a for a, _ in pairs], t)

            @pl.when(s <= zp)
            def _():
                tile(s, pick([b for _, b in pairs], t), any(a == 0 for a, _ in pairs))

            return carry

        lax.fori_loop(0, len(pairs), visit, 0)

    def arrive(s):
        c_kzr(s).wait_recv()
        pass_on(s)

    def ready(s):
        c_kd(s).wait_recv()

    def halves(p):
        w_all(qb.at[1:3, p], r_q.at[p])
        for i in (0, 1):
            c_qh(i, p).start()

    def give(s):
        for k in (1, 0):
            rot = turned[s, :, 128 * k : 128 * k + 128].T
            part[s, k, :, 512:WIDE] = jnp.concatenate([rot, jnp.zeros((128, 64), F32)], axis=1)
            if k == 1:
                c_d(s).start()

    ready(0)
    run((0, 0))
    c_q(1, 1).start()
    c_q(2, 1).start()
    pl.semaphore_wait(hop.at[0], 6)
    relay(1)
    have(1, arrive)
    have(1, ready)
    run((1, 0))
    halves(0)
    w_all(st.at[1:3], r_st.at[0])
    c_st(3).start()
    project(1)
    run((0, 1), (1, 1))
    pl.semaphore_wait(hop.at[1], 2)
    relay(2)
    halves(1)
    project(2)
    run((0, 2))
    have(2, arrive)
    run((1, 2))
    have(2, ready)
    run((2, 0), (2, 1))
    pl.semaphore_wait(hop.at[2], 2)
    pl.semaphore_signal(hop.at[3], inc=1, device_id=sib, device_id_type=MESH)
    w_all(qb.at[3], r_q.at[2])
    c_st(3).wait_recv()
    project(3)
    run((2, 3))
    have(3, arrive)
    run((1, 3))
    have(1, give)
    run((0, 3))
    give(0)
    have(3, ready)
    run((3, 3))
    do_dq(3)
    c_dh(0).start()
    c_dh(1).start()
    have(1, do_y1)
    run((3, 1))
    do_y1(0)

    def do_term(p, slots, fresh):
        for k in (0, 1):
            got = jnp.zeros((512, 128), F32)
            for j in slots:
                slot, b = place_of(j, 2 * p + k)
                m = mix[slot, 0:512, b * 128 : b * 128 + 128]
                high = m.astype(BF16)
                rest = (m - high.astype(F32)).astype(BF16)
                q = qb[j, p, :, k * 128 : k * 128 + 128]
                got = got + dot(jnp.concatenate([high, rest], axis=1), jnp.concatenate([q, q], axis=0))
            got = (factor * got).reshape(16, 4, 8, 128)
            if not fresh:
                got = got + term[p, :, :, :, k * 128 : (k + 1) * 128]
            term[p, :, :, :, k * 128 : (k + 1) * 128] = got

    def hand_over(core):
        @pl.when(c == core)
        def _():
            for j in (3, 1, 2, 0):
                c_t(j).start()

    do_term(0, (1, 2, 3), True)
    run((3, 0))
    do_term(0, (0,), False)
    hand_over(1)
    do_term(1, (0, 3), True)
    run((3, 2))
    have(3, give)
    run((2, 2))
    do_term(1, (1, 2), False)
    hand_over(0)

    def over_x(core):
        @pl.when(c == core)
        def _():
            for j in (3, 1, 2, 0):
                turn = (x, x1, x3, x2)[j]
                c_t(j).wait_recv()
                got = (term[core, :, turn] + termr[:, turn]).reshape(128, 256)
                if j == 0:
                    wx0[...] = got
                else:
                    wxs[j] = got.astype(BF16)
                    c_wx(j).start()

    over_x(0)
    have(3, do_y1)
    have(2, give)
    have(1, do_y2)
    over_x(1)
    have(2, do_y1)
    do_y2(0)
    do_dq(1)
    do_dq(2)
    have(3, do_y2)
    have(1, do_z)

    pl.semaphore_wait(hop.at[3], 1)
    got = wx0[...]
    w_all(wxr.at[1:4], r_wx.at[0])
    for j in (1, 2, 3):
        got = got + wxr[j].astype(F32)
    got = got.reshape(16, 8, 256)
    for k in (0, 1):
        rows = slice(4 * k, 4 * k + 4)
        wz[16 * k : 16 * k + 16] = jnp.concatenate([got[:, rows, 0:128], got[:, rows, 128:256]], axis=1)
    far_first = (8, 7, 9, 6, 10, 5, 11, 4, 12, 3, 13, 2, 14, 1, 15)
    for d in far_first:
        for k in (0, 1):
            c_wz(k, d).start()
    c_wz(1, 0).start()
    have(3, do_z)
    have(2, do_y2)

    c_dh(1).wait_recv()
    dqs[1, 64:128, :] += dqh[1]
    c_dq(1).start()
    c_dh(0).wait_recv()
    dqs[2, 0:64, :] += dqh[0]
    c_dq(2).start()
    do_z(0)
    do_dq(0)
    have(2, do_z)

    def wait_z(d, carry):
        c_zr(d).wait_recv()
        zs[0] += zr[d]
        return carry

    lax.fori_loop(1, more + 1, wait_z, 0)
    fin[0] = zs[0].astype(BF16)
    for j in (1, 2, 3):
        c_f(j).start()

    def drain(s):
        if s < 3:

            @pl.when(more > 0)
            def _():
                c_kz(s).wait_send()

        c_kd(s).wait_send()
        c_d(s).wait_send()
        w_all(y1s.at[s], s_y1.at[s])
        w_all(y2s.at[s], s_y2.at[s])
        if s > 0:
            c_z(s).wait_send()

    for s in range(4):
        have(s, drain)
    w_all(qb.at[0:2], s_q.at[0])
    w_all(qb.at[0], s_q.at[1])
    w_all(st.at[1:3], s_st.at[0])
    c_st(3).wait_send()
    w_all(dqs.at[3], s_dh.at[0])
    w_all(termr, s_t.at[0])
    w_all(wxs.at[1:4], s_wx.at[0])

    w_all(dqr, r_dq.at[0])
    o_main[...] = dqs[0, :, 0:512] + dqr[0, :, 0:512] + dqr[1, :, 0:512]
    o_rot[...] = dqs[0, :, 512:768] + dqr[0, :, 512:768] + dqr[1, :, 512:768]

    w_all(fin.at[1:4], r_f.at[0])
    for j in range(4):
        rows = pl.ds(pl.multiple_of((y, y1, y3, y2)[j] * 32, 32), 32)
        got = zs[0] if j == 0 else fin[j].astype(F32)
        o_lat[rows, :] = got[:, 0:512]
        krots[rows, :] = got[:, 512:640]
    o_krot[...] = krots[...].T[0:64, :]
    w_all(dqs.at[1:3], s_dq.at[0])
    w_all(fin.at[1:4], s_f.at[0])
    w_all(wz.at[1:32], s_wz.at[0])

    w_all(wzr.at[1:32], r_wz.at[0])
    sums = [wz[16 * c + z] + wzr[1:16].sum(axis=0), wzr[16:32].sum(axis=0)]
    for core in (0, 1):

        @pl.when(c == core)
        def _(core=core):
            for k, at in ((0, core), (1, 1 - core)):
                o_weight[:, 256 * at : 256 * at + 128] = sums[k][0:4, :]
                o_weight[:, 256 * at + 128 : 256 * at + 256] = sums[k][4:8, :]


def put_out(*refs):
    ends, sems = refs[5:10], refs[10]
    copies = [pltpu.make_async_copy(a, b, sems.at[i]) for i, (a, b) in enumerate(zip(refs[:5], ends))]
    for copy in copies:
        copy.start()
    for copy in copies:
        copy.wait()


def per_device(query_main, query_rotary, latent, key_rotary, key_weight, value_weight, head_output, output_grad, row_logsum):
    v = pl.BlockSpec(memory_space=pltpu.VMEM)
    hbm = pl.BlockSpec(memory_space=pl.ANY)
    dma = pltpu.SemaphoreType.DMA
    scratch = [
        pltpu.VMEM((128, 128), F32),
        pltpu.VMEM((2, 512, 512), BF16),
        pltpu.VMEM((128, 512), BF16),
        pltpu.VMEM((4, 128), F32),
        pltpu.VMEM((64, 128), BF16),
        pltpu.VMEM((4, 2, 128, 640), BF16),
        pltpu.VMEM((4, 8, 512), F32),
        pltpu.VMEM((4, 8, 512), F32),
        pltpu.VMEM((4, 512, WIDE), BF16),
        pltpu.VMEM((4, 64, 512), BF16),
        pltpu.VMEM((4, 512, 512), BF16),
        pltpu.VMEM((4, 2, 128, WIDE), BF16),
        pltpu.VMEM((4, WIDE, 512), F32),
        pltpu.VMEM((4, 2, 128, WIDE), F32),
        pltpu.VMEM((4, 64, 256), F32),
        pltpu.VMEM((4, 128, WIDE), F32),
        pltpu.VMEM((4, 2, 2, 16, WIDE), BF16),
        pltpu.VMEM((4, 2, 2, 16, WIDE), BF16),
        pltpu.VMEM((4, 2, 16, WIDE), F32),
        pltpu.VMEM((4, 2, 16, WIDE), F32),
        pltpu.VMEM((4, 32, WIDE), F32),
        pltpu.VMEM((4, 32, WIDE), F32),
        pltpu.VMEM((4, 32, WIDE), BF16),
        pltpu.VMEM((4, 128, 768), F32),
        pltpu.VMEM((2, 64, 768), F32),
        pltpu.VMEM((2, 128, 768), F32),
        pltpu.VMEM((2, 16, 4, 8, 256), F32),
        pltpu.VMEM((16, 4, 8, 256), F32),
        pltpu.VMEM((128, 256), F32),
        pltpu.VMEM((4, 128, 256), BF16),
        pltpu.VMEM((4, 128, 256), BF16),
        pltpu.VMEM((32, 8, 128), F32),
        pltpu.VMEM((32, 8, 128), F32),
        dma((6,)),
        pltpu.SemaphoreType.REGULAR((4,)),
        dma((2,)), dma((3,)),
        dma((2,)), dma((2,)),
        dma((3,)), dma((3,)),
        dma((4,)), dma((4,)),
        dma((4,)), dma((4,)),
        dma((4,)), dma((4,)),
        dma((4,)), dma((4,)),
        dma((3,)), dma((3,)),
        dma((1,)), dma((1,)),
        dma((1,)), dma((2,)),
        dma((1,)), dma((1,)),
        dma((1,)), dma((4,)),
        dma((1,)), dma((1,)),
        dma((1,)), dma((1,)),
    ]
    got = pl.pallas_call(
        body,
        out_shape=(
            pltpu.VMEM((128, 512), F32),
            pltpu.VMEM((128, 256), F32),
            pltpu.VMEM((128, 512), F32),
            pltpu.VMEM((64, 128), F32),
            pltpu.VMEM((4, 512), F32),
        ),
        in_specs=[hbm] * 9,
        out_specs=(v,) * 5,
        scratch_shapes=scratch,
        compiler_params=pltpu.CompilerParams(
            collective_id=0, has_side_effects=True, vmem_limit_bytes=56 * 1024 * 1024
        ),
    )(query_main, query_rotary, latent, key_rotary.T, key_weight, value_weight, head_output, output_grad, row_logsum)
    main, rot, lat, krot, weight = pl.pallas_call(
        put_out,
        out_shape=(
            jax.ShapeDtypeStruct((128, 512), F32),
            jax.ShapeDtypeStruct((128, 256), F32),
            jax.ShapeDtypeStruct((128, 512), F32),
            jax.ShapeDtypeStruct((64, 128), F32),
            jax.ShapeDtypeStruct((4, 512), F32),
        ),
        in_specs=[v] * 5,
        out_specs=(hbm,) * 5,
        scratch_shapes=[dma((5,))],
    )(*(pltpu.with_memory_space_constraint(a, pltpu.VMEM) for a in got))
    return main, rot, lat, krot.T, weight


def solution(mesh):
    finer = Mesh(mesh.devices.reshape(16, 4, 2, mesh.shape["tp"]), ("z", "x", "c", "y"))
    return jax.shard_map(
        per_device,
        mesh=finer,
        in_specs=(
            P(SP, "y"),
            P(SP, "y"),
            P(SP, None),
            P(SP, None),
            P(None, "y"),
            P(None, "y"),
            P(SP, "y"),
            P(SP, "y"),
            P("y", SP),
        ),
        out_specs=(P(SP, "y"), P(SP, "y"), P(SP, None), P(SP, None), P(SP, "y")),
        check_vma=False,
    )
```

```python
import jax
import jax.numpy as jnp
from jax import lax
from jax.experimental import pallas as pl
from jax.experimental.pallas import tpu as pltpu
from jax.sharding import Mesh
from jax.sharding import PartitionSpec as P

MESH = pl.DeviceIdType.MESH
SP = ("z", "x", "c")
F32 = jnp.float32
BF16 = jnp.bfloat16
WIDE = 640
LOG2E = 1.4426950408889634
NT = (((1,), (1,)), ((), ()))
TN = (((0,), (0,)), ((), ()))


def dot(a, b, dims=(((1,), (0,)), ((), ()))):
    return lax.dot_general(a, b, dims, preferred_element_type=F32)


def pick(table, t):
    out = jnp.int32(0)
    for k, v in enumerate(table):
        if v:
            out = out + jnp.where(t == k, v, 0)
    return out


def body(
    qm, qr, lat, krt, kwh, vwh, hoh, og, lsh,
    o_main, o_rot, o_lat, o_krot, o_weight,
    krots, kv, ho, ls, krv, qb, st, sts, qc, qt, gr, keys, mix, part, turned, dsum, y1s, y1r, y2s, y2r, zs, zr, fin,
    dqs, dqh, dqr, term, termr, wx0, wxs, wxr, wz, wzr,
    s_loc, hop, s_q, r_q, s_st, r_st, s_kz, r_kz, s_kd, r_kd, s_d, r_d, s_y1, r_y1, s_y2, r_y2,
    s_z, r_z, s_f, r_f, s_dh, r_dh, s_dq, r_dq, s_t, r_t, s_wx, r_wx, s_wz, r_wz,
):
    z, x, c, y = (lax.axis_index(a) for a in ("z", "x", "c", "y"))
    factor = 192.0 ** (-0.5)
    zp = jnp.where(z < 3, z, (z + 1) % 4)
    planes = jnp.where(z < 3, 3, jnp.where(z < 15, 4, 1))
    more = planes - 1 - zp
    sib = {"c": 1 - c}
    x1, x3, x2 = x + 1 - 2 * (x % 2), 3 - x, (x + 2) % 4
    y1, y3, y2 = y + 1 - 2 * (y % 2), 3 - y, (y + 2) % 4
    xdev = (None, {"x": x1}, {"x": x3}, {"x": x2})
    ydev = (None, {"y": y1}, {"y": y3}, {"y": y2})

    def remote(src, dst, ss, rs, dev):
        return pltpu.make_async_remote_copy(
            src_ref=src, dst_ref=dst, send_sem=ss, recv_sem=rs, device_id=dev, device_id_type=MESH
        )

    def c_q(j, p):
        return remote(qb.at[0, p], qb.at[j, p], s_q.at[0], r_q.at[p], xdev[j])

    def c_qh(i, p):
        rows = pl.ds(64 * i, 64)
        return remote(qb.at[1 + i, p, rows], qb.at[3, p, rows], s_q.at[1], r_q.at[2], xdev[2 - i])

    def c_st(j):
        if j == 3:
            return remote(st.at[1], st.at[3], s_st.at[1], r_st.at[1], xdev[2])
        return remote(st.at[0], st.at[j], s_st.at[0], r_st.at[0], xdev[j])

    def c_kz(s):
        return remote(keys.at[s, 0], keys.at[s + 1, 0], s_kz.at[s], r_kz.at[s], {"z": z + 1})

    def c_kzr(s):
        return remote(keys.at[s - 1, 0], keys.at[s, 0], s_kz.at[s - 1], r_kz.at[s - 1], {"z": z - 1})

    def c_kd(s):
        return remote(keys.at[s, 0], keys.at[s, 1], s_kd.at[s], r_kd.at[s], sib)

    def c_d(s):
        return remote(part.at[s, 1], dsum.at[s], s_d.at[s], r_d.at[s], sib)

    def c_y1(s, g):
        return remote(y1s.at[s, g], y1r.at[s, g], s_y1.at[s], r_y1.at[s], ydev[1 + g])

    def c_y2(s, g):
        return remote(y2s.at[s, g], y2r.at[s, g], s_y2.at[s], r_y2.at[s], ydev[2 - g])

    def c_z(s):
        return remote(zs.at[s], zr.at[s], s_z.at[s - 1], r_z.at[s - 1], {"z": z - s})

    def c_zr(s):
        return remote(zs.at[s], zr.at[s], s_z.at[s - 1], r_z.at[s - 1], {"z": z + s})

    def c_f(j):
        return remote(fin.at[0], fin.at[j], s_f.at[0], r_f.at[0], ydev[j])

    def c_dh(i):
        rows = pl.ds(64 * i, 64)
        return remote(dqs.at[3, rows], dqh.at[i], s_dh.at[0], r_dh.at[i], xdev[1 + i])

    def c_dq(j):
        return remote(dqs.at[j], dqr.at[j - 1], s_dq.at[0], r_dq.at[0], xdev[j])

    def c_t(j):
        turn = (x, x1, x3, x2)[j]
        return remote(term.at[1 - c, :, turn], termr.at[:, turn], s_t.at[0], r_t.at[j], sib)

    def c_wx(j):
        return remote(wxs.at[j], wxr.at[j], s_wx.at[0], r_wx.at[0], xdev[j])

    def c_wz(k, d):
        to = (z + d) % 16
        own = c if k == 0 else 1 - c
        dev = {"z": to, "c": own}
        return remote(wz.at[own * 16 + to], wzr.at[16 * k + d], s_wz.at[0], r_wz.at[0], dev)

    def w_all(ref, sem):
        pltpu.make_async_copy(ref, ref, sem).wait()

    barrier = pltpu.get_barrier_semaphore()
    for dev in (sib, *xdev[1:3], *ydev[1:3], {"z": (z + 1) % 16}, {"z": (z + 15) % 16}):
        pl.semaphore_signal(barrier, inc=1, device_id=dev, device_id_type=MESH)
    first = [
        (krt, krv, 0),
        (lat, keys.at[0, 0, :, 0:512], 1),
        (qm.at[:, 0:256], qb.at[0, 0, :, 0:256], 2),
        (qr.at[:, 0:128], qb.at[0, 0, :, 256:384], 2),
        (og.at[:, 0:256], qb.at[0, 0, :, 384:640], 2),
        (qm.at[:, 256:512], qb.at[0, 1, :, 0:256], 2),
        (qr.at[:, 128:256], qb.at[0, 1, :, 256:384], 2),
        (og.at[:, 256:512], qb.at[0, 1, :, 384:640], 2),
        (kwh, kv.at[0], 3),
        (vwh, kv.at[1], 3),
        (hoh, ho, 4),
        (lsh, ls, 5),
    ]
    kw, vw = kv.at[0], kv.at[1]
    loads = [pltpu.make_async_copy(a, b, s_loc.at[i]) for a, b, i in first]
    for copy in loads:
        copy.start()
    loads[0].wait()
    keys[0, 0, :, 512:WIDE] = jnp.concatenate([krv[...].T, jnp.zeros((128, 64), BF16)], axis=1)
    loads[1].wait()
    w_all(qb.at[0], s_loc.at[2])
    pl.semaphore_wait(barrier, 7)

    def relay(i):
        for d in (1 << i, 16 - (1 << i)):
            pl.semaphore_signal(hop.at[i], inc=1, device_id={"z": (z + d) % 16}, device_id_type=MESH)
        if i == 0:
            for dev in (*xdev[1:3], *ydev[1:3]):
                pl.semaphore_signal(hop.at[i], inc=1, device_id=dev, device_id_type=MESH)

    def pass_on(s):
        if s < 3:

            @pl.when(more > 0)
            def _():
                c_kz(s).start()

        c_kd(s).start()

    c_q(1, 0).start()
    c_q(2, 0).start()
    pass_on(0)
    relay(0)

    def rows_of(slot):
        if slot in (0, 3):
            return [(slot, h) for h in range(4)]
        return [(j, 2 * (slot - 1) + h) for j in (1, 2) for h in (0, 1)]

    def place_of(j, h):
        if j in (0, 3):
            return j, h
        return 1 + h // 2, 2 * (j - 1) + h % 2

    w_all(kv, s_loc.at[3])
    for copy in loads[10:]:
        copy.wait()
    ones = jnp.ones((8, 128), F32)
    for h in range(4):
        cols = pl.ds(h * 128, 128)
        prod = ho[:, cols].astype(F32) * qb[0, h // 2, :, 384 + h % 2 * 128 : 512 + h % 2 * 128].astype(F32)
        sums = lax.dot_general(
            ones, prod, NT, precision=lax.Precision.HIGHEST, preferred_element_type=F32
        )
        st[0, 1:2, cols] = sums[0:1, :]
        st[0, 0:1, cols] = LOG2E * ls[h : h + 1, :]
    for j in (1, 2):
        c_st(j).start()

    def project(slot):
        for b, (j, h) in enumerate(rows_of(slot)):
            p, k = h // 2, h % 2
            cols = pl.ds(h * 128, 128)
            rows = pl.ds(b * 128, 128)
            qc[slot, rows, 0:512] = dot(qb[j, p, :, k * 128 : k * 128 + 128], kw[:, cols], NT).astype(BF16)
            gr[slot, rows, :] = dot(qb[j, p, :, 384 + k * 128 : 512 + k * 128], vw[:, cols], NT).astype(BF16)
            rot = qb[j, p, :, 256 + k * 64 : 320 + k * 64]
            qt[slot, :, rows] = rot.T
            qc[slot, rows, 512:WIDE] = jnp.concatenate([rot, jnp.zeros((128, 64), BF16)], axis=1)
            sts[slot, 0:2, rows] = st[j, 0:2, cols]

    project(0)
    mix[...] = jnp.zeros_like(mix)
    part[...] = jnp.zeros_like(part)
    turned[...] = jnp.zeros_like(turned)

    def tile(s, j, masked):
        kt = keys[s].reshape(256, WIDE)
        turn_a = jnp.where(j == 0, x, jnp.where(j == 3, x2, x1))
        turn_b = jnp.where(j == 0, x, jnp.where(j == 3, x2, x3))
        far = jnp.where(s > 0, 1 << 20, 0)
        first = (2 * x + c) * 128 - far
        second = (2 * x + 1 - c) * 128 - 128 - far
        k_row = lax.broadcasted_iota(jnp.int32, (256, 1), 0)
        k_place = jnp.where(k_row < 128, k_row + first, k_row + second)
        q_col = lax.broadcasted_iota(jnp.int32, (1, 512), 1)
        q_place = q_col % 128 + jnp.where(q_col < 256, 2 * turn_a + c, 2 * turn_b + c) * 128
        scores = dot(kt, qc[j], NT)
        weights = jnp.exp2((factor * LOG2E) * scores - sts[j, 0:1, :])
        if masked:
            weights = jnp.where(k_place <= q_place, weights, 0.0)
        slopes = dot(kt[:, 0:512], gr[j], NT)
        dscores = weights * (slopes - sts[j, 1:2, :])
        w_low = weights.astype(BF16)
        d_low = dscores.astype(BF16)
        mix[j, 0:576, :] += dot(kt[:, 0:576], d_low, TN)
        main = factor * dot(d_low, qc[j, :, 0:512]) + dot(w_low, gr[j])
        part[s, :, :, 0:512] += main.reshape(2, 128, 512)
        turned[s] += factor * dot(qt[j], d_low, NT)

    def own(s, g, yy):
        rows = pl.ds(pl.multiple_of(yy * 32 + 16 * g, 16), 16)
        return part[s, 0, rows, :] + dsum[s, rows, :]

    def do_y1(s):
        c_d(s).wait_recv()
        for g in (0, 1):
            y1s[s, g, 0] = own(s, g, (y1, y3)[g]).astype(BF16)
            y1s[s, g, 1] = own(s, g, y2).astype(BF16)
            c_y1(s, g).start()

    def do_y2(s):
        w_all(y1r.at[s], r_y1.at[s])
        for g in (0, 1):
            y2s[s, g] = own(s, g, (y3, y1)[g]) + y1r[s, g, 1].astype(F32)
            c_y2(s, g).start()

    def do_z(s):
        w_all(y2r.at[s], r_y2.at[s])
        for g in (0, 1):
            zs[s, 16 * g : 16 * g + 16, :] = own(s, g, y) + y1r[s, g, 0].astype(F32) + y2r[s, g]
        if s > 0:
            c_z(s).start()

    def have(s, act):
        @pl.when(zp >= s)
        def _():
            act(s)

    def do_dq(j):
        for h in range(4):
            cols = pl.ds(h * 128, 128)
            slot, b = place_of(j, h)
            m = mix[slot, 0:512, b * 128 : b * 128 + 128]
            high = m.astype(BF16)
            rest = (m - high.astype(F32)).astype(BF16)
            got = dot(high, kw[:, cols], TN) + dot(rest, kw[:, cols], TN)
            dqs[j, :, cols] = factor * got
        for g in range(2):
            pair = []
            for h in (2 * g, 2 * g + 1):
                slot, b = place_of(j, h)
                pair.append(mix[slot, 512:640, b * 128 : b * 128 + 128].T[:, 0:64])
            dqs[j, :, 512 + g * 128 : 640 + g * 128] = factor * jnp.concatenate(pair, axis=1)

    def run(*pairs):
        def visit(t, carry):
            s = pick([a for a, _ in pairs], t)

            @pl.when(s <= zp)
            def _():
                tile(s, pick([b for _, b in pairs], t), any(a == 0 for a, _ in pairs))

            return carry

        lax.fori_loop(0, len(pairs), visit, 0)

    def arrive(s):
        c_kzr(s).wait_recv()
        pass_on(s)

    def ready(s):
        c_kd(s).wait_recv()

    def halves(p):
        w_all(qb.at[1:3, p], r_q.at[p])
        for i in (0, 1):
            c_qh(i, p).start()

    def give(s):
        for k in (1, 0):
            rot = turned[s, :, 128 * k : 128 * k + 128].T
            part[s, k, :, 512:WIDE] = jnp.concatenate([rot, jnp.zeros((128, 64), F32)], axis=1)
            if k == 1:
                c_d(s).start()

    ready(0)
    run((0, 0))
    c_q(1, 1).start()
    c_q(2, 1).start()
    pl.semaphore_wait(hop.at[0], 6)
    relay(1)
    have(1, arrive)
    have(1, ready)
    run((1, 0))
    halves(0)
    w_all(st.at[1:3], r_st.at[0])
    c_st(3).start()
    project(1)
    run((0, 1), (1, 1))
    pl.semaphore_wait(hop.at[1], 2)
    relay(2)
    halves(1)
    project(2)
    run((0, 2))
    have(2, arrive)
    run((1, 2))
    have(2, ready)
    run((2, 0), (2, 1))
    pl.semaphore_wait(hop.at[2], 2)
    pl.semaphore_signal(hop.at[3], inc=1, device_id=sib, device_id_type=MESH)
    w_all(qb.at[3], r_q.at[2])
    c_st(3).wait_recv()
    project(3)
    run((2, 3))
    have(3, arrive)
    run((1, 3))
    have(1, give)
    run((0, 3))
    give(0)
    have(3, ready)
    run((3, 3))
    do_dq(3)
    c_dh(0).start()
    c_dh(1).start()
    have(1, do_y1)
    run((3, 1))

    def do_term(p, slots, fresh):
        for k in (0, 1):
            got = jnp.zeros((512, 128), F32)
            for j in slots:
                slot, b = place_of(j, 2 * p + k)
                m = mix[slot, 0:512, b * 128 : b * 128 + 128]
                high = m.astype(BF16)
                rest = (m - high.astype(F32)).astype(BF16)
                q = qb[j, p, :, k * 128 : k * 128 + 128]
                got = got + dot(jnp.concatenate([high, rest], axis=1), jnp.concatenate([q, q], axis=0))
            got = (factor * got).reshape(16, 4, 8, 128)
            if not fresh:
                got = got + term[p, :, :, :, k * 128 : (k + 1) * 128]
            term[p, :, :, :, k * 128 : (k + 1) * 128] = got

    def hand_over(core):
        @pl.when(c == core)
        def _():
            for j in (3, 1, 2, 0):
                c_t(j).start()

    do_term(0, (1, 2, 3), True)
    run((3, 0))
    do_term(0, (0,), False)
    hand_over(1)
    do_term(1, (0, 3), True)
    run((3, 2))
    have(3, give)
    run((2, 2))
    do_term(1, (1, 2), False)
    hand_over(0)

    def over_x(core):
        @pl.when(c == core)
        def _():
            for j in (3, 1, 2, 0):
                turn = (x, x1, x3, x2)[j]
                c_t(j).wait_recv()
                got = (term[core, :, turn] + termr[:, turn]).reshape(128, 256)
                if j == 0:
                    wx0[...] = got
                else:
                    wxs[j] = got.astype(BF16)
                    c_wx(j).start()

    over_x(0)
    have(3, do_y1)
    have(2, give)
    have(1, do_y2)
    over_x(1)
    have(2, do_y1)
    do_y1(0)
    do_dq(1)
    do_dq(2)
    have(3, do_y2)
    have(1, do_z)

    pl.semaphore_wait(hop.at[3], 1)
    got = wx0[...]
    w_all(wxr.at[1:4], r_wx.at[0])
    for j in (1, 2, 3):
        got = got + wxr[j].astype(F32)
    got = got.reshape(16, 8, 256)
    for k in (0, 1):
        rows = slice(4 * k, 4 * k + 4)
        wz[16 * k : 16 * k + 16] = jnp.concatenate([got[:, rows, 0:128], got[:, rows, 128:256]], axis=1)
    far_first = (8, 7, 9, 6, 10, 5, 11, 4, 12, 3, 13, 2, 14, 1, 15)
    for d in far_first:
        for k in (0, 1):
            c_wz(k, d).start()
    c_wz(1, 0).start()
    have(3, do_z)
    have(2, do_y2)
    do_y2(0)

    c_dh(1).wait_recv()
    dqs[1, 64:128, :] += dqh[1]
    c_dq(1).start()
    c_dh(0).wait_recv()
    dqs[2, 0:64, :] += dqh[0]
    c_dq(2).start()
    do_dq(0)
    have(2, do_z)
    do_z(0)

    def wait_z(d, carry):
        c_zr(d).wait_recv()
        zs[0] += zr[d]
        return carry

    lax.fori_loop(1, more + 1, wait_z, 0)
    fin[0] = zs[0].astype(BF16)
    for j in (1, 2, 3):
        c_f(j).start()

    def drain(s):
        if s < 3:

            @pl.when(more > 0)
            def _():
                c_kz(s).wait_send()

        c_kd(s).wait_send()
        c_d(s).wait_send()
        w_all(y1s.at[s], s_y1.at[s])
        w_all(y2s.at[s], s_y2.at[s])
        if s > 0:
            c_z(s).wait_send()

    for s in range(4):
        have(s, drain)
    w_all(qb.at[0:2], s_q.at[0])
    w_all(qb.at[0], s_q.at[1])
    w_all(st.at[1:3], s_st.at[0])
    c_st(3).wait_send()
    w_all(dqs.at[3], s_dh.at[0])
    w_all(termr, s_t.at[0])
    w_all(wxs.at[1:4], s_wx.at[0])

    w_all(dqr, r_dq.at[0])
    o_main[...] = dqs[0, :, 0:512] + dqr[0, :, 0:512] + dqr[1, :, 0:512]
    o_rot[...] = dqs[0, :, 512:768] + dqr[0, :, 512:768] + dqr[1, :, 512:768]

    w_all(fin.at[1:4], r_f.at[0])
    for j in range(4):
        rows = pl.ds(pl.multiple_of((y, y1, y3, y2)[j] * 32, 32), 32)
        got = zs[0] if j == 0 else fin[j].astype(F32)
        o_lat[rows, :] = got[:, 0:512]
        krots[rows, :] = got[:, 512:640]
    o_krot[...] = krots[...].T[0:64, :]
    w_all(dqs.at[1:3], s_dq.at[0])
    w_all(fin.at[1:4], s_f.at[0])
    w_all(wz.at[1:32], s_wz.at[0])

    w_all(wzr.at[1:32], r_wz.at[0])
    sums = [wz[16 * c + z] + wzr[1:16].sum(axis=0), wzr[16:32].sum(axis=0)]
    for core in (0, 1):

        @pl.when(c == core)
        def _(core=core):
            for k, at in ((0, core), (1, 1 - core)):
                o_weight[:, 256 * at : 256 * at + 128] = sums[k][0:4, :]
                o_weight[:, 256 * at + 128 : 256 * at + 256] = sums[k][4:8, :]


def put_out(*refs):
    ends, sems = refs[5:10], refs[10]
    copies = [pltpu.make_async_copy(a, b, sems.at[i]) for i, (a, b) in enumerate(zip(refs[:5], ends))]
    for copy in copies:
        copy.start()
    for copy in copies:
        copy.wait()


def per_device(query_main, query_rotary, latent, key_rotary, key_weight, value_weight, head_output, output_grad, row_logsum):
    v = pl.BlockSpec(memory_space=pltpu.VMEM)
    hbm = pl.BlockSpec(memory_space=pl.ANY)
    dma = pltpu.SemaphoreType.DMA
    scratch = [
        pltpu.VMEM((128, 128), F32),
        pltpu.VMEM((2, 512, 512), BF16),
        pltpu.VMEM((128, 512), BF16),
        pltpu.VMEM((4, 128), F32),
        pltpu.VMEM((64, 128), BF16),
        pltpu.VMEM((4, 2, 128, 640), BF16),
        pltpu.VMEM((4, 8, 512), F32),
        pltpu.VMEM((4, 8, 512), F32),
        pltpu.VMEM((4, 512, WIDE), BF16),
        pltpu.VMEM((4, 64, 512), BF16),
        pltpu.VMEM((4, 512, 512), BF16),
        pltpu.VMEM((4, 2, 128, WIDE), BF16),
        pltpu.VMEM((4, WIDE, 512), F32),
        pltpu.VMEM((4, 2, 128, WIDE), F32),
        pltpu.VMEM((4, 64, 256), F32),
        pltpu.VMEM((4, 128, WIDE), F32),
        pltpu.VMEM((4, 2, 2, 16, WIDE), BF16),
        pltpu.VMEM((4, 2, 2, 16, WIDE), BF16),
        pltpu.VMEM((4, 2, 16, WIDE), F32),
        pltpu.VMEM((4, 2, 16, WIDE), F32),
        pltpu.VMEM((4, 32, WIDE), F32),
        pltpu.VMEM((4, 32, WIDE), F32),
        pltpu.VMEM((4, 32, WIDE), BF16),
        pltpu.VMEM((4, 128, 768), F32),
        pltpu.VMEM((2, 64, 768), F32),
        pltpu.VMEM((2, 128, 768), F32),
        pltpu.VMEM((2, 16, 4, 8, 256), F32),
        pltpu.VMEM((16, 4, 8, 256), F32),
        pltpu.VMEM((128, 256), F32),
        pltpu.VMEM((4, 128, 256), BF16),
        pltpu.VMEM((4, 128, 256), BF16),
        pltpu.VMEM((32, 8, 128), F32),
        pltpu.VMEM((32, 8, 128), F32),
        dma((6,)),
        pltpu.SemaphoreType.REGULAR((4,)),
        dma((2,)), dma((3,)),
        dma((2,)), dma((2,)),
        dma((3,)), dma((3,)),
        dma((4,)), dma((4,)),
        dma((4,)), dma((4,)),
        dma((4,)), dma((4,)),
        dma((4,)), dma((4,)),
        dma((3,)), dma((3,)),
        dma((1,)), dma((1,)),
        dma((1,)), dma((2,)),
        dma((1,)), dma((1,)),
        dma((1,)), dma((4,)),
        dma((1,)), dma((1,)),
        dma((1,)), dma((1,)),
    ]
    got = pl.pallas_call(
        body,
        out_shape=(
            pltpu.VMEM((128, 512), F32),
            pltpu.VMEM((128, 256), F32),
            pltpu.VMEM((128, 512), F32),
            pltpu.VMEM((64, 128), F32),
            pltpu.VMEM((4, 512), F32),
        ),
        in_specs=[hbm] * 9,
        out_specs=(v,) * 5,
        scratch_shapes=scratch,
        compiler_params=pltpu.CompilerParams(
            collective_id=0, has_side_effects=True, vmem_limit_bytes=56 * 1024 * 1024
        ),
    )(query_main, query_rotary, latent, key_rotary.T, key_weight, value_weight, head_output, output_grad, row_logsum)
    main, rot, lat, krot, weight = pl.pallas_call(
        put_out,
        out_shape=(
            jax.ShapeDtypeStruct((128, 512), F32),
            jax.ShapeDtypeStruct((128, 256), F32),
            jax.ShapeDtypeStruct((128, 512), F32),
            jax.ShapeDtypeStruct((64, 128), F32),
            jax.ShapeDtypeStruct((4, 512), F32),
        ),
        in_specs=[v] * 5,
        out_specs=(hbm,) * 5,
        scratch_shapes=[dma((5,))],
    )(*(pltpu.with_memory_space_constraint(a, pltpu.VMEM) for a in got))
    return main, rot, lat, krot.T, weight


def solution(mesh):
    finer = Mesh(mesh.devices.reshape(16, 4, 2, mesh.shape["tp"]), ("z", "x", "c", "y"))
    return jax.shard_map(
        per_device,
        mesh=finer,
        in_specs=(
            P(SP, "y"),
            P(SP, "y"),
            P(SP, None),
            P(SP, None),
            P(None, "y"),
            P(None, "y"),
            P(SP, "y"),
            P(SP, "y"),
            P("y", SP),
        ),
        out_specs=(P(SP, "y"), P(SP, "y"), P(SP, None), P(SP, None), P(SP, "y")),
        check_vma=False,
    )
```
